512 devices in a mesh: fs: 128 (over z, x, core), tp: 4 (over y).
Axes of the slice: x: 4, y: 4, z: 16, core: 2. Of those that a mesh axis runs over, the one named last changes fastest.
Arguments:
- layer_input: bfloat16 [98304, 2048], P('fs'), may hold values from -6 to 6
- branch_cotangent: bfloat16 [98304, 1024], P('fs', 'tp'), may hold values from -0.014343262 to 0.014343262
- gate_cotangent: bfloat16 [98304, 1024], P('fs', 'tp'), may hold values from -0.014343262 to 0.014343262
- branch_factor: bfloat16 [2048, 128], P('fs'), may hold values from -0.5 to 0.5
- gate_factor: bfloat16 [2048, 128], P('fs'), may hold values from -0.5 to 0.5
- branch_weight: float32 [2048, 1024], P('fs', 'tp'), may hold values from -6 to 6
- gate_weight: float32 [2048, 1024], P('fs', 'tp'), may hold values from -6 to 6
- branch_first: float32 [128, 1024], P(None, 'tp'), may hold values from -6 to 6
- gate_first: float32 [128, 1024], P(None, 'tp'), may hold values from -6 to 6
- branch_second: float32 [128, 1024], P(None, 'tp'), may hold values from 0.0625 to 900
- gate_second: float32 [128, 1024], P(None, 'tp'), may hold values from 0.0625 to 900
Outputs:
- branch_step: float32 [2048, 1024], P('fs', 'tp')
- gate_step: float32 [2048, 1024], P('fs', 'tp')
- branch_new: float32 [2048, 1024], P('fs', 'tp')
- gate_new: float32 [2048, 1024], P('fs', 'tp')
- branch_copy: bfloat16 [2048, 1024], P(None, 'tp')
- gate_copy: bfloat16 [2048, 1024], P(None, 'tp')
- branch_first_new: float32 [128, 1024], P(None, 'tp')
- gate_first_new: float32 [128, 1024], P(None, 'tp')
- branch_second_new: float32 [128, 1024], P(None, 'tp')
- gate_second_new: float32 [128, 1024], P(None, 'tp')
The draws below stay inside these ranges and needn't reach their ends.
All inputs are finite; a program needn't handle non-finite values.
Results may differ from the reference program's by a relative error of at most 0.00055.
Values may be sent and summed in bfloat16 or wider, within the bound.
No kernel may reach another device: no remote copies, remote signals or barrier semaphores. Data moves between devices by JAX's collectives and lax.ppermute only.
A program may use at most 64 MiB of HBM per device.

```python
import jax
import jax.numpy as jnp
from jax import lax

D = 2048
W = 1024
RANK = 128
TOKENS = 98304


def second_moment(key, marker):
    base_key = jax.random.fold_in(key, marker)
    row_key, col_key, noise_key = jax.random.split(base_key, 3)
    columns = jnp.arange(W, dtype=jnp.float32) / (W - 1)
    col_scale = jnp.exp(1.2 * (1.0 - columns)) * jax.random.uniform(col_key, (W,), jnp.float32, 1.0, 3.0)
    row_scale = jax.random.uniform(row_key, (RANK,), jnp.float32, 1.0, 3.0)
    noise = jnp.exp(jax.random.uniform(noise_key, (RANK, W), jnp.float32, jnp.log(0.5), jnp.log(2.0)))
    outer = row_scale[:, None] * col_scale[None, :]
    return (0.25 * noise * outer * outer).astype(jnp.float32)


def draw_branch_second(key, part):
    return second_moment(key, 11)


def draw_gate_second(key, part):
    return second_moment(key, 12)


def level_of(stream_key, extent, shards, smallest, largest):
    gain = 1.0
    for axis_at, parts in shards:
        heights = jax.random.uniform(jax.random.fold_in(jax.random.fold_in(stream_key, 6), axis_at), (parts,), jnp.float32, smallest / len(shards), largest / len(shards))
        gain = gain * jnp.repeat(jnp.exp(heights), extent[axis_at] // parts).reshape((-1,) + (1,) * (len(extent) - 1 - axis_at))
    return gain


def gaussian(rng, dims, width, bound, pieces=(), kind=jnp.bfloat16):
    values = jax.random.normal(rng, dims, jnp.float32) * width
    if len(pieces) > 0:
        values = level_of(rng, dims, pieces, -0.22, 0.18) * values
    return jnp.clip(values, min=-bound, max=bound).astype(kind)


def setup_inputs(seed: int = 0) -> dict:
    arg_keys = jax.random.split(jax.random.key(seed), 12)
    layer_input = gaussian(arg_keys[0], (TOKENS, D), 1.0, 6.0, ((0, 128),))
    branch_cotangent = gaussian(arg_keys[1], (TOKENS, W), (0.75 * TOKENS ** -0.5), 0.014343262, ((0, 128), (1, 4)))
    gate_cotangent = gaussian(arg_keys[2], (TOKENS, W), (0.75 * TOKENS ** -0.5), 0.014343262, ((0, 128), (1, 4)))
    branch_factor = gaussian(arg_keys[3], (D, RANK), RANK ** -0.5, 0.5, ((0, 128),))
    gate_factor = gaussian(arg_keys[4], (D, RANK), RANK ** -0.5, 0.5, ((0, 128),))
    branch_weight = gaussian(arg_keys[5], (D, W), 1.0, 6.0, ((0, 128), (1, 4)), jnp.float32)
    gate_weight = gaussian(arg_keys[6], (D, W), 1.0, 6.0, ((0, 128), (1, 4)), jnp.float32)
    branch_first = gaussian(arg_keys[7], (RANK, W), 1.0, 6.0, ((1, 4),), jnp.float32)
    gate_first = gaussian(arg_keys[8], (RANK, W), 1.0, 6.0, ((1, 4),), jnp.float32)
    branch_second = draw_branch_second(jax.random.fold_in(arg_keys[11], 71), 0)
    gate_second = draw_gate_second(jax.random.fold_in(arg_keys[11], 71), 0)
    return dict(layer_input=layer_input, branch_cotangent=branch_cotangent, gate_cotangent=gate_cotangent, branch_factor=branch_factor, gate_factor=gate_factor, branch_weight=branch_weight, gate_weight=gate_weight, branch_first=branch_first, gate_first=gate_first, branch_second=branch_second, gate_second=gate_second)


first_decay = 0.8
second_decay = 0.9
learn_rate = 0.5

def reference(layer_input, branch_cotangent, gate_cotangent, branch_factor, gate_factor, branch_weight, gate_weight, branch_first, gate_first, branch_second, gate_second):
    highest = lax.Precision.HIGHEST
    groups = ((branch_cotangent, branch_factor, branch_first, branch_second), (gate_cotangent, gate_factor, gate_first, gate_second))
    firsts_new = []
    seconds_new = []
    directions = []
    sum_squares = jnp.zeros((), jnp.float32)
    for cotangent, factor, first_old, second_old in groups:
        gradient = jnp.dot(layer_input.T, cotangent, preferred_element_type=jnp.float32)
        projected = jnp.dot(factor.astype(jnp.float32).T, gradient, precision=highest)
        first_new = first_decay * first_old + (1.0 - first_decay) * projected
        second_new = second_decay * second_old + (1.0 - second_decay) * projected * projected
        direction = first_new / jnp.sqrt(second_new)
        sum_squares = sum_squares + jnp.sum(direction * direction)
        firsts_new.append(first_new)
        seconds_new.append(second_new)
        directions.append(direction)
    step_scale = learn_rate / jnp.sqrt(sum_squares / (2 * RANK * W) + 1e-06)
    branch_step = -step_scale * jnp.dot(branch_factor.astype(jnp.float32), directions[0], precision=highest)
    gate_step = -step_scale * jnp.dot(gate_factor.astype(jnp.float32), directions[1], precision=highest)
    branch_new = branch_weight + branch_step
    gate_new = gate_weight + gate_step
    return (branch_step, gate_step, branch_new, gate_new, branch_new.astype(jnp.bfloat16), gate_new.astype(jnp.bfloat16), firsts_new[0], firsts_new[1], seconds_new[0], seconds_new[1])
```

```python
import jax
import jax.numpy as jnp
from jax import lax
from jax.sharding import Mesh
from jax.sharding import PartitionSpec as P

FS = ("zh", "zl", "x", "c")
Z = ("zh", "zl")

first_decay = 0.8
second_decay = 0.9
learn_rate = 0.5


def exchanged(blocks, axes):
    return lax.all_to_all(blocks, axes, split_axis=0, concat_axis=0, tiled=True)


def from_everyone(x, axes):
    peers = 1
    for a in axes:
        peers *= lax.axis_size(a)
    return exchanged(jnp.broadcast_to(x, (peers, *x.shape)), axes)


def whole_factors(branch_factor, gate_factor):
    rows, rank = branch_factor.shape
    half = rows // 2
    quarters = jnp.stack(
        [branch_factor[:half], branch_factor[half:], gate_factor[:half], gate_factor[half:]]
    )
    mine = lax.dynamic_index_in_dim(quarters, lax.axis_index("tp"), 0, keepdims=False)
    along_z = from_everyone(mine, Z)
    along_plane = from_everyone(along_z, ("x", "tp"))
    both = from_everyone(along_plane, ("c",))
    nz = along_z.shape[0]
    nx = lax.axis_size("x")
    parts = both.reshape(2, nx, 2, 2, nz, half, rank)
    return parts.transpose(4, 1, 0, 3, 5, 2, 6).reshape(nz * nx * 2 * rows, 2 * rank)


def two_parts(x):
    high = lax.reduce_precision(x, 8, 7)
    return high.astype(jnp.bfloat16), (x - high).astype(jnp.bfloat16)


def projected_locally(rows, cotangent):
    high, low = two_parts(rows)
    rank = rows.shape[1]
    both = lax.dot_general(
        jnp.concatenate([high, low], axis=1),
        cotangent,
        (((0,), (0,)), ((), ())),
        preferred_element_type=jnp.float32,
    )
    return both[:rank] + both[rank:]


def summed_over_fs(branch_local, gate_local):
    mine = exchanged(jnp.stack([branch_local, gate_local]), ("c",)).sum(axis=0)
    rank, width = mine.shape
    near = lax.axis_size("zl") * lax.axis_size("x")
    piece = exchanged(mine.reshape(near, rank // near, width), ("zl", "x")).sum(axis=0)
    total = from_everyone(piece, ("zh",)).sum(axis=0)
    whole = from_everyone(total, ("zl", "x")).reshape(rank, width)
    both = from_everyone(whole, ("c",))
    return both[0], both[1]


def update_moments(projected, first_old, second_old):
    first_new = first_decay * first_old + (1.0 - first_decay) * projected
    second_new = second_decay * second_old + (1.0 - second_decay) * projected * projected
    return (first_new, second_new, first_new / jnp.sqrt(second_new))


def times_direction(factor, direction):
    high = lax.reduce_precision(direction, 8, 7)
    rest = direction - high
    middle = lax.reduce_precision(rest, 8, 7)
    low = rest - middle
    width = direction.shape[1]
    parts = jnp.concatenate([p.astype(jnp.bfloat16) for p in (high, middle, low)], axis=1)
    out = jnp.dot(factor, parts, preferred_element_type=jnp.float32)
    return out[:, :width] + (out[:, width : 2 * width] + out[:, 2 * width :])


def whole_copies(branch_new, gate_new):
    mine = jnp.concatenate([branch_new, gate_new], axis=1).astype(jnp.bfloat16)
    rows, width = mine.shape
    along_z = from_everyone(mine, Z)
    along_x = from_everyone(along_z, ("x",))
    both = from_everyone(along_x, ("c",))
    whole = both.transpose(2, 1, 0, 3, 4).reshape(-1, width)
    return whole[:, : width // 2], whole[:, width // 2 :]


def local(
    layer_input,
    branch_cotangent,
    gate_cotangent,
    branch_factor,
    gate_factor,
    branch_weight,
    gate_weight,
    branch_first,
    gate_first,
    branch_second,
    gate_second,
):
    rank, width = branch_first.shape
    factors = whole_factors(branch_factor, gate_factor)
    rows = jnp.dot(layer_input, factors, preferred_element_type=jnp.float32)
    branch_local = projected_locally(rows[:, :rank], branch_cotangent)
    gate_local = projected_locally(rows[:, rank:], gate_cotangent)
    branch_projected, gate_projected = summed_over_fs(branch_local, gate_local)
    branch_first_new, branch_second_new, branch_direction = update_moments(
        branch_projected, branch_first, branch_second
    )
    gate_first_new, gate_second_new, gate_direction = update_moments(
        gate_projected, gate_first, gate_second
    )
    local_squares = jnp.sum(branch_direction * branch_direction) + jnp.sum(
        gate_direction * gate_direction
    )
    squares = from_everyone(jnp.full((1, 128), local_squares), ("tp",))
    sum_squares = jnp.sum(squares, axis=0)[0, 0]
    entries = 2 * rank * width * lax.axis_size("tp")
    step_scale = learn_rate / jnp.sqrt(sum_squares / entries + 1e-06)
    branch_step = -step_scale * times_direction(branch_factor, branch_direction)
    gate_step = -step_scale * times_direction(gate_factor, gate_direction)
    branch_new = branch_weight + branch_step
    gate_new = gate_weight + gate_step
    branch_copy, gate_copy = whole_copies(branch_new, gate_new)
    return (
        branch_step,
        gate_step,
        branch_new,
        gate_new,
        branch_copy,
        gate_copy,
        branch_first_new,
        gate_first_new,
        branch_second_new,
        gate_second_new,
    )


def solution(mesh):
    finer = Mesh(
        mesh.devices.reshape(8, 2, 4, 2, mesh.shape["tp"]), ("zh", "zl", "x", "c", "tp")
    )
    sharded = P(FS, None)
    split = P(FS, "tp")
    kept = P(None, "tp")
    in_specs = (sharded, split, split, sharded, sharded, split, split, kept, kept, kept, kept)
    out_specs = (split, split, split, split, kept, kept, kept, kept, kept, kept)
    return jax.shard_map(local, mesh=finer, in_specs=in_specs, out_specs=out_specs, check_vma=False)
```

```python
import jax
import jax.numpy as jnp
from jax import lax
from jax.sharding import Mesh
from jax.sharding import PartitionSpec as P

FS = ("zh", "zl", "x", "c")

first_decay = 0.8
second_decay = 0.9
learn_rate = 0.5


def exchanged(blocks, axes):
    return lax.all_to_all(blocks, axes, split_axis=0, concat_axis=0, tiled=True)


def from_everyone(x, axes):
    peers = 1
    for a in axes:
        peers *= lax.axis_size(a)
    return exchanged(jnp.broadcast_to(x, (peers, *x.shape)), axes)


NEAR = ("zl", "x")


def gathered(block):
    along_far = from_everyone(block, ("zh",))
    along_near = from_everyone(along_far, NEAR)
    mine = along_near.reshape(lax.axis_size("zl"), lax.axis_size("x"), *along_far.shape)
    other = lax.ppermute(mine, "c", [(0, 1), (1, 0)])
    core = lax.axis_index("c")
    return jnp.stack([jnp.where(core == 0, mine, other), jnp.where(core == 0, other, mine)])


def in_row_order(blocks):
    return blocks.transpose(3, 1, 2, 0, 4, 5).reshape(-1, blocks.shape[-1])


def two_parts(x):
    high = lax.reduce_precision(x, 8, 7)
    return high.astype(jnp.bfloat16), (x - high).astype(jnp.bfloat16)


def projected_locally(rows, cotangent):
    high, low = two_parts(rows)
    rank = rows.shape[1]
    both = lax.dot_general(
        jnp.concatenate([high, low], axis=1),
        cotangent,
        (((0,), (0,)), ((), ())),
        preferred_element_type=jnp.float32,
    )
    return both[:rank] + both[rank:]


def summed_over_fs(branch_local, gate_local):
    both = jnp.stack([branch_local, gate_local])
    group = ("zl", "x", "c")
    peers = lax.axis_size("zl") * lax.axis_size("x") * lax.axis_size("c")
    pieces = both.reshape(peers, -1, both.shape[-1])
    piece = exchanged(pieces, group).sum(axis=0)
    total = from_everyone(piece, ("zh",)).sum(axis=0)
    whole = from_everyone(total, group).reshape(both.shape)
    return whole[0], whole[1]


def update_moments(projected, first_old, second_old):
    first_new = first_decay * first_old + (1.0 - first_decay) * projected
    second_new = second_decay * second_old + (1.0 - second_decay) * projected * projected
    return (first_new, second_new, first_new / jnp.sqrt(second_new))


def times_direction(factor, direction):
    high = lax.reduce_precision(direction, 8, 7)
    rest = direction - high
    middle = lax.reduce_precision(rest, 8, 7)
    low = rest - middle
    width = direction.shape[1]
    parts = jnp.concatenate([p.astype(jnp.bfloat16) for p in (high, middle, low)], axis=1)
    out = jnp.dot(factor, parts, preferred_element_type=jnp.float32)
    return out[:, :width] + (out[:, width : 2 * width] + out[:, 2 * width :])


def local(
    layer_input,
    branch_cotangent,
    gate_cotangent,
    branch_factor,
    gate_factor,
    branch_weight,
    gate_weight,
    branch_first,
    gate_first,
    branch_second,
    gate_second,
):
    rank, width = branch_first.shape
    factors = in_row_order(gathered(jnp.concatenate([branch_factor, gate_factor], axis=1)))
    rows = jnp.dot(layer_input, factors, preferred_element_type=jnp.float32)
    branch_local = projected_locally(rows[:, :rank], branch_cotangent)
    gate_local = projected_locally(rows[:, rank:], gate_cotangent)
    branch_projected, gate_projected = summed_over_fs(branch_local, gate_local)
    branch_first_new, branch_second_new, branch_direction = update_moments(
        branch_projected, branch_first, branch_second
    )
    gate_first_new, gate_second_new, gate_direction = update_moments(
        gate_projected, gate_first, gate_second
    )
    local_squares = jnp.sum(branch_direction * branch_direction) + jnp.sum(
        gate_direction * gate_direction
    )
    squares = from_everyone(jnp.full((1, 128), local_squares), ("tp",))
    sum_squares = jnp.sum(squares, axis=0)[0, 0]
    entries = 2 * rank * width * lax.axis_size("tp")
    step_scale = learn_rate / jnp.sqrt(sum_squares / entries + 1e-06)
    branch_step = -step_scale * times_direction(branch_factor, branch_direction)
    gate_step = -step_scale * times_direction(gate_factor, gate_direction)
    branch_new = branch_weight + branch_step
    gate_new = gate_weight + gate_step
    copies = in_row_order(
        gathered(jnp.concatenate([branch_new, gate_new], axis=1).astype(jnp.bfloat16))
    )
    branch_copy, gate_copy = copies[:, :width], copies[:, width:]
    return (
        branch_step,
        gate_step,
        branch_new,
        gate_new,
        branch_copy,
        gate_copy,
        branch_first_new,
        gate_first_new,
        branch_second_new,
        gate_second_new,
    )


def solution(mesh):
    finer = Mesh(
        mesh.devices.reshape(8, 2, 4, 2, mesh.shape["tp"]), ("zh", "zl", "x", "c", "tp")
    )
    sharded = P(FS, None)
    split = P(FS, "tp")
    kept = P(None, "tp")
    in_specs = (sharded, split, split, sharded, sharded, split, split, kept, kept, kept, kept)
    out_specs = (split, split, split, split, kept, kept, kept, kept, kept, kept)
    return jax.shard_map(local, mesh=finer, in_specs=in_specs, out_specs=out_specs, check_vma=False)
```

```python
import functools

import jax
import jax.numpy as jnp
from jax import lax
from jax.experimental import pallas as pl
from jax.experimental.pallas import tpu as pltpu
from jax.sharding import Mesh
from jax.sharding import PartitionSpec as P

FS = ("zh", "zl", "x", "c")
FAR = ("zh",)
NEAR = ("zl", "x")
NEAR_CORES = ("zl", "x", "c")

first_decay = 0.8
second_decay = 0.9
learn_rate = 0.5


def size_of(axes):
    peers = 1
    for a in axes:
        peers *= lax.axis_size(a)
    return peers


def exchanged(blocks, axes):
    return lax.all_to_all(blocks, axes, split_axis=0, concat_axis=0, tiled=True)


def from_everyone(x, axes):
    return exchanged(jnp.broadcast_to(x, (size_of(axes), *x.shape)), axes)


def in_row_order(blocks):
    return blocks.transpose(3, 1, 2, 0, 4, 5).reshape(-1, blocks.shape[-1])


def two_parts(x):
    high = lax.reduce_precision(x, 8, 7)
    return high.astype(jnp.bfloat16), (x - high).astype(jnp.bfloat16)


def projected_locally(rows, cotangent):
    high, low = two_parts(rows)
    rank = rows.shape[1]
    both = lax.dot_general(
        jnp.concatenate([high, low], axis=1),
        cotangent,
        (((0,), (0,)), ((), ())),
        preferred_element_type=jnp.float32,
    )
    return both[:rank] + both[rank:]


def moments_kernel(
    projected,
    branch_first,
    gate_first,
    branch_second,
    gate_second,
    branch_first_new,
    gate_first_new,
    branch_second_new,
    gate_second_new,
    parts,
    squares,
):
    rank, width = branch_first.shape
    total = jnp.zeros((8, 128), jnp.float32)
    both = (
        (branch_first, branch_second, branch_first_new, branch_second_new),
        (gate_first, gate_second, gate_first_new, gate_second_new),
    )
    for p, (first, second, first_new, second_new) in enumerate(both):
        r = projected[p]
        moved = first_decay * first[...] + (1.0 - first_decay) * r
        spread = second_decay * second[...] + (1.0 - second_decay) * r * r
        first_new[...] = moved
        second_new[...] = spread
        direction = moved / jnp.sqrt(spread)
        high = direction.astype(jnp.bfloat16)
        rest = direction - high.astype(jnp.float32)
        middle = rest.astype(jnp.bfloat16)
        low = (rest - middle.astype(jnp.float32)).astype(jnp.bfloat16)
        parts[p, :, :width] = high
        parts[p, :, width : 2 * width] = middle
        parts[p, :, 2 * width :] = low
        squared = direction * direction
        for column in range(0, width, 128):
            total += jnp.sum(
                squared[:, column : column + 128].reshape(rank // 8, 8, 128), axis=0
            )
    for peer in range(squares.shape[0]):
        squares[peer] = total


def rows_kernel(
    entries,
    squares,
    parts,
    factors,
    arrived,
    rows_new,
    branch_step,
    gate_step,
    branch_new,
    gate_new,
    steps_all,
):
    block, width = branch_step.shape
    far = factors.shape[0]
    rank = parts.shape[1]
    at = lax.axis_index("zh")
    total = jnp.sum(jnp.sum(squares[...], axis=0), keepdims=True)
    minus_scale = -learn_rate / jnp.sqrt(total / entries + 1e-06)
    steps = (branch_step, gate_step)
    news = (branch_new, gate_new)
    for p in range(2):
        factor = factors[:, :, p * rank : (p + 1) * rank].reshape(far * block, rank)
        out = jnp.dot(factor, parts[p], preferred_element_type=jnp.float32)
        raw = out[:, :width] + (out[:, width : 2 * width] + out[:, 2 * width :])
        step = (minus_scale * raw).reshape(far, block, width)
        weights = arrived[:, (p + 1) * block : (p + 2) * block, :]
        rows_new[:, :, p * width : (p + 1) * width] = (weights + step).astype(jnp.bfloat16)
        steps_all[...] = step
        mine = steps_all[at]
        steps[p][...] = mine
        news[p][...] = arrived[at, (p + 1) * block : (p + 2) * block, :] + mine


def whole():
    return pl.BlockSpec(memory_space=pltpu.VMEM)


def outgoing_kernel(pieces, branch_weight, gate_weight, blocks):
    height = pieces.shape[1]
    block = branch_weight.shape[0]
    piece = jnp.sum(pieces[...], axis=0)
    for peer in range(blocks.shape[0]):
        blocks[peer, :height] = piece
        blocks[peer, height : height + block] = branch_weight[...]
        blocks[peer, height + block :] = gate_weight[...]


def copies_kernel(mine, other, branch_copy, gate_copy):
    near_z, near_x, far, block, _ = mine.shape
    width = branch_copy.shape[1]
    core = lax.axis_index("c")
    for f in range(far):
        for z in range(near_z):
            for x in range(near_x):
                row = ((f * near_z + z) * near_x + x) * 2 * block
                for source, place in ((mine, core), (other, 1 - core)):
                    rows = pl.ds(pl.multiple_of(row + place * block, block), block)
                    branch_copy[rows, :] = source[z, x, f, :, :width]
                    gate_copy[rows, :] = source[z, x, f, :, width:]


def outgoing(pieces, branch_weight, gate_weight, peers):
    height = pieces.shape[1] + 2 * branch_weight.shape[0]
    return pl.pallas_call(
        outgoing_kernel,
        out_shape=jax.ShapeDtypeStruct((peers, height, pieces.shape[2]), jnp.float32),
        in_specs=[whole()] * 3,
        out_specs=whole(),
        compiler_params=pltpu.CompilerParams(vmem_limit_bytes=4 << 20),
        name="outgoing",
    )(pieces, branch_weight, gate_weight)


def whole_copies(mine, other):
    near_z, near_x, far, block, columns = mine.shape
    copy = jax.ShapeDtypeStruct((2 * near_z * near_x * far * block, columns // 2), jnp.bfloat16)
    return pl.pallas_call(
        copies_kernel,
        out_shape=[copy, copy],
        in_specs=[whole()] * 2,
        out_specs=[whole()] * 2,
        compiler_params=pltpu.CompilerParams(vmem_limit_bytes=8 << 20),
        name="whole_copies",
    )(mine, other)


def moments(projected, branch_first, gate_first, branch_second, gate_second, planes):
    rank, width = branch_first.shape
    f32 = jax.ShapeDtypeStruct((rank, width), jnp.float32)
    return pl.pallas_call(
        moments_kernel,
        out_shape=[
            f32,
            f32,
            f32,
            f32,
            jax.ShapeDtypeStruct((2, rank, 3 * width), jnp.bfloat16),
            jax.ShapeDtypeStruct((planes, 8, 128), jnp.float32),
        ],
        in_specs=[whole()] * 5,
        out_specs=[whole()] * 6,
        compiler_params=pltpu.CompilerParams(vmem_limit_bytes=6 << 20),
        name="moments",
    )(projected, branch_first, gate_first, branch_second, gate_second)


def new_rows(entries, squares, parts, factors, arrived, block, width):
    far = factors.shape[0]
    f32 = jax.ShapeDtypeStruct((block, width), jnp.float32)
    return pl.pallas_call(
        functools.partial(rows_kernel, entries),
        out_shape=[jax.ShapeDtypeStruct((far, block, 2 * width), jnp.bfloat16), f32, f32, f32, f32],
        in_specs=[whole()] * 4,
        out_specs=[whole()] * 5,
        scratch_shapes=[pltpu.VMEM((far, block, width), jnp.float32)],
        compiler_params=pltpu.CompilerParams(vmem_limit_bytes=6 << 20),
        name="new_rows",
    )(squares, parts, factors, arrived)


def local(
    layer_input,
    branch_cotangent,
    gate_cotangent,
    branch_factor,
    gate_factor,
    branch_weight,
    gate_weight,
    branch_first,
    gate_first,
    branch_second,
    gate_second,
):
    rank, width = branch_first.shape
    block = branch_weight.shape[0]
    near = (lax.axis_size("zl"), lax.axis_size("x"))

    far_factors = from_everyone(jnp.concatenate([branch_factor, gate_factor], axis=1), FAR)
    near_factors = from_everyone(far_factors, NEAR)
    all_factors = from_everyone(near_factors, ("c",))
    factors = in_row_order(all_factors.reshape(2, *near, *far_factors.shape))

    rows = jnp.dot(layer_input, factors, preferred_element_type=jnp.float32)
    both = jnp.stack(
        [
            projected_locally(rows[:, :rank], branch_cotangent),
            projected_locally(rows[:, rank:], gate_cotangent),
        ]
    )
    pieces = both.reshape(size_of(NEAR_CORES), -1, width)
    height = pieces.shape[1]
    blocks = outgoing(
        exchanged(pieces, NEAR_CORES), branch_weight, gate_weight, size_of(FAR)
    )
    arrived = exchanged(blocks, FAR)
    total = arrived[:, :height].sum(axis=0)
    projected = from_everyone(total, NEAR_CORES).reshape(both.shape)

    planes = lax.axis_size("tp")
    (
        branch_first_new,
        gate_first_new,
        branch_second_new,
        gate_second_new,
        parts,
        squares,
    ) = moments(projected, branch_first, gate_first, branch_second, gate_second, planes)
    squares = exchanged(squares, ("tp",))
    rows_new, branch_step, gate_step, branch_new, gate_new = new_rows(
        2 * rank * width * planes,
        squares,
        parts,
        far_factors,
        arrived,
        block,
        width,
    )

    mine = from_everyone(rows_new, NEAR).reshape(*near, *rows_new.shape)
    other = lax.ppermute(mine, "c", [(0, 1), (1, 0)])
    branch_copy, gate_copy = whole_copies(mine, other)
    return (
        branch_step,
        gate_step,
        branch_new,
        gate_new,
        branch_copy,
        gate_copy,
        branch_first_new,
        gate_first_new,
        branch_second_new,
        gate_second_new,
    )


def solution(mesh):
    finer = Mesh(
        mesh.devices.reshape(8, 2, 4, 2, mesh.shape["tp"]), ("zh", "zl", "x", "c", "tp")
    )
    sharded = P(FS, None)
    split = P(FS, "tp")
    kept = P(None, "tp")
    in_specs = (sharded, split, split, sharded, sharded, split, split, kept, kept, kept, kept)
    out_specs = (split, split, split, split, kept, kept, kept, kept, kept, kept)
    return jax.shard_map(local, mesh=finer, in_specs=in_specs, out_specs=out_specs, check_vma=False)
```

```python
import functools

import jax
import jax.numpy as jnp
from jax import lax
from jax.experimental import pallas as pl
from jax.experimental.pallas import tpu as pltpu
from jax.sharding import Mesh
from jax.sharding import PartitionSpec as P


FS = ("zh", "zl", "x", "c")
FAR = ("zh",)
NEAR = ("zl", "x")
NEAR_CORES = ("zl", "x", "c")

first_decay = 0.8
second_decay = 0.9
learn_rate = 0.5


def size_of(axes):
    peers = 1
    for a in axes:
        peers *= lax.axis_size(a)
    return peers


def exchanged(blocks, axes):
    return lax.all_to_all(blocks, axes, split_axis=0, concat_axis=0, tiled=True)


def from_everyone(x, axes):
    return exchanged(jnp.broadcast_to(x, (size_of(axes), *x.shape)), axes)


def swapped(x):
    return lax.ppermute(x, "c", [(0, 1), (1, 0)])


def two_parts(x):
    high = lax.reduce_precision(x, 8, 7)
    return high.astype(jnp.bfloat16), (x - high).astype(jnp.bfloat16)


def projected_locally(rows, cotangent):
    high, low = two_parts(rows)
    rank = rows.shape[1]
    both = lax.dot_general(
        jnp.concatenate([high, low], axis=1),
        cotangent,
        (((0,), (0,)), ((), ())),
        preferred_element_type=jnp.float32,
    )
    return both[:rank] + both[rank:]


def moved_and_spread(projected, first, second):
    moved = first_decay * first + (1.0 - first_decay) * projected
    spread = second_decay * second + (1.0 - second_decay) * projected * projected
    return moved, spread


def direction_kernel(
    projected, branch_first, gate_first, branch_second, gate_second, parts, squares
):
    rank, width = branch_first.shape
    total = jnp.zeros((8, 128), jnp.float32)
    both = ((branch_first, branch_second), (gate_first, gate_second))
    for p, (first, second) in enumerate(both):
        moved, spread = moved_and_spread(projected[p], first[...], second[...])
        direction = moved / jnp.sqrt(spread)
        high = direction.astype(jnp.bfloat16)
        rest = direction - high.astype(jnp.float32)
        middle = rest.astype(jnp.bfloat16)
        low = (rest - middle.astype(jnp.float32)).astype(jnp.bfloat16)
        parts[p, :, :width] = high
        parts[p, :, width : 2 * width] = middle
        parts[p, :, 2 * width :] = low
        squared = direction * direction
        for column in range(0, width, 128):
            total += jnp.sum(
                squared[:, column : column + 128].reshape(rank // 8, 8, 128), axis=0
            )
    squares[...] = total


def scale_of(entries, squares):
    total = jnp.sum(jnp.sum(squares, axis=0), keepdims=True)
    return -learn_rate / jnp.sqrt(total / entries + 1e-06)


def times_parts(factor, parts):
    width = parts.shape[1] // 3
    out = jnp.dot(factor, parts, preferred_element_type=jnp.float32)
    return out[:, :width] + (out[:, width : 2 * width] + out[:, 2 * width :])


def rows_kernel(entries, squares, parts, factors, arrived, rows_new):
    far, block, _ = factors.shape
    rank = parts.shape[1]
    width = arrived.shape[2]
    minus_scale = scale_of(entries, squares[...])
    for p in range(2):
        factor = factors[:, :, p * rank : (p + 1) * rank].reshape(far * block, rank)
        step = (minus_scale * times_parts(factor, parts[p])).reshape(far, block, width)
        weights = arrived[:, (p + 1) * block : (p + 2) * block, :]
        rows_new[:, :, p * width : (p + 1) * width] = (weights + step).astype(jnp.bfloat16)


def results_kernel(
    entries,
    projected,
    branch_first,
    gate_first,
    branch_second,
    gate_second,
    squares,
    parts,
    branch_factor,
    gate_factor,
    branch_weight,
    gate_weight,
    branch_step,
    gate_step,
    branch_new,
    gate_new,
    branch_first_new,
    gate_first_new,
    branch_second_new,
    gate_second_new,
):
    minus_scale = scale_of(entries, squares[...])
    both = (
        (branch_first, branch_second, branch_first_new, branch_second_new),
        (gate_first, gate_second, gate_first_new, gate_second_new),
    )
    for p, (first, second, first_new, second_new) in enumerate(both):
        moved, spread = moved_and_spread(projected[p], first[...], second[...])
        first_new[...] = moved
        second_new[...] = spread
    rows = (
        (branch_factor, branch_weight, branch_step, branch_new),
        (gate_factor, gate_weight, gate_step, gate_new),
    )
    for p, (factor, weight, step_out, new_out) in enumerate(rows):
        step = minus_scale * times_parts(factor[...], parts[p])
        step_out[...] = step
        new_out[...] = weight[...] + step


def outgoing_kernel(pieces, branch_weight, gate_weight, outgoing_block):
    height = pieces.shape[1]
    block = branch_weight.shape[0]
    outgoing_block[:height] = jnp.sum(pieces[...], axis=0)
    outgoing_block[height : height + block] = branch_weight[...]
    outgoing_block[height + block :] = gate_weight[...]


def factors_kernel(mine, other, factors):
    near_z, near_x, far, block, _ = mine.shape
    core = lax.axis_index("c")
    for f in range(far):
        for z in range(near_z):
            for x in range(near_x):
                row = ((f * near_z + z) * near_x + x) * 2 * block
                for source, place in ((mine, core), (other, 1 - core)):
                    rows = pl.ds(pl.multiple_of(row + place * block, block), block)
                    factors[rows, :] = source[z, x, f]


def placed(blocks, place, copies, done):
    near_z, near_x = blocks.shape[:2]
    width = copies[0].shape[-1]
    started = []
    for p, copy in enumerate(copies):
        for z in range(near_z):
            for x in range(near_x):
                started.append(
                    pltpu.make_async_copy(
                        blocks.at[z, x, :, :, pl.ds(p * width, width)],
                        copy.at[:, z, x, place],
                        done.at[len(started)],
                    )
                )
    for one in started:
        one.start()
    for one in started:
        one.wait()


def mine_kernel(mine, branch_copy, gate_copy, done):
    placed(mine, lax.axis_index("c"), (branch_copy, gate_copy), done)


def other_kernel(other, branch_in, gate_in, branch_copy, gate_copy, done):
    del branch_in, gate_in
    placed(other, 1 - lax.axis_index("c"), (branch_copy, gate_copy), done)


def whole():
    return pl.BlockSpec(memory_space=pltpu.VMEM)


def anywhere():
    return pl.BlockSpec(memory_space=pl.ANY)


def grant(mib):
    return pltpu.CompilerParams(vmem_limit_bytes=mib << 20)


def outgoing(pieces, branch_weight, gate_weight):
    height = pieces.shape[1] + 2 * branch_weight.shape[0]
    return pl.pallas_call(
        outgoing_kernel,
        out_shape=jax.ShapeDtypeStruct((height, pieces.shape[2]), jnp.float32),
        in_specs=[whole()] * 3,
        out_specs=whole(),
        compiler_params=grant(4),
        name="outgoing",
    )(pieces, branch_weight, gate_weight)


def whole_factors(mine, other):
    near_z, near_x, far, block, columns = mine.shape
    return pl.pallas_call(
        factors_kernel,
        out_shape=jax.ShapeDtypeStruct((2 * near_z * near_x * far * block, columns), mine.dtype),
        in_specs=[whole()] * 2,
        out_specs=whole(),
        compiler_params=grant(4),
        name="whole_factors",
    )(mine, other)


def copies_of(mine):
    near_z, near_x, far, block, columns = mine.shape
    copy = jax.ShapeDtypeStruct((far, near_z, near_x, 2, block, columns // 2), mine.dtype)
    return [copy, copy], [pltpu.SemaphoreType.DMA((2 * near_z * near_x,))]


def place_mine(mine):
    shapes, scratch = copies_of(mine)
    return pl.pallas_call(
        mine_kernel,
        out_shape=shapes,
        in_specs=[whole()],
        out_specs=[anywhere()] * 2,
        scratch_shapes=scratch,
        compiler_params=grant(4),
        cost_estimate=pl.CostEstimate(flops=1 << 20, bytes_accessed=1 << 21, transcendentals=0),
        name="place_mine",
    )(mine)


def place_other(other, branch_copy, gate_copy):
    shapes, scratch = copies_of(other)
    return pl.pallas_call(
        other_kernel,
        out_shape=shapes,
        in_specs=[whole(), anywhere(), anywhere()],
        out_specs=[anywhere()] * 2,
        scratch_shapes=scratch,
        input_output_aliases={1: 0, 2: 1},
        compiler_params=grant(4),
        name="place_other",
    )(other, branch_copy, gate_copy)


def directions(projected, branch_first, gate_first, branch_second, gate_second):
    rank, width = branch_first.shape
    return pl.pallas_call(
        direction_kernel,
        out_shape=[
            jax.ShapeDtypeStruct((2, rank, 3 * width), jnp.bfloat16),
            jax.ShapeDtypeStruct((8, 128), jnp.float32),
        ],
        in_specs=[whole()] * 5,
        out_specs=[whole()] * 2,
        compiler_params=grant(6),
        name="directions",
    )(projected, branch_first, gate_first, branch_second, gate_second)


def new_rows(entries, squares, parts, factors, arrived):
    far, block, _ = factors.shape
    return pl.pallas_call(
        functools.partial(rows_kernel, entries),
        out_shape=jax.ShapeDtypeStruct((far, block, 2 * arrived.shape[2]), jnp.bfloat16),
        in_specs=[whole()] * 4,
        out_specs=whole(),
        compiler_params=grant(6),
        name="new_rows",
    )(squares, parts, factors, arrived)


def results(entries, projected, moments, squares, parts, factors, weights):
    rank, width = moments[0].shape
    block = weights[0].shape[0]
    row = jax.ShapeDtypeStruct((block, width), jnp.float32)
    moment = jax.ShapeDtypeStruct((rank, width), jnp.float32)
    return pl.pallas_call(
        functools.partial(results_kernel, entries),
        out_shape=[row] * 4 + [moment] * 4,
        in_specs=[whole()] * 11,
        out_specs=[whole()] * 8,
        compiler_params=grant(6),
        cost_estimate=pl.CostEstimate(flops=1 << 22, bytes_accessed=1 << 21, transcendentals=0),
        name="results",
    )(projected, *moments, squares, parts, *factors, *weights)


def body(
    layer_input,
    branch_cotangent,
    gate_cotangent,
    branch_factor,
    gate_factor,
    branch_weight,
    gate_weight,
    branch_first,
    gate_first,
    branch_second,
    gate_second,
):
    rank, width = branch_first.shape
    near = (lax.axis_size("zl"), lax.axis_size("x"))

    far_factors = from_everyone(jnp.concatenate([branch_factor, gate_factor], axis=1), FAR)
    near_factors = from_everyone(far_factors, NEAR).reshape(*near, *far_factors.shape)
    factors = whole_factors(near_factors, swapped(near_factors))

    rows = jnp.dot(layer_input, factors, preferred_element_type=jnp.float32)
    both = jnp.stack(
        [
            projected_locally(rows[:, :rank], branch_cotangent),
            projected_locally(rows[:, rank:], gate_cotangent),
        ]
    )
    pieces = both.reshape(size_of(NEAR_CORES), -1, width)
    height = pieces.shape[1]
    outgoing_block = outgoing(exchanged(pieces, NEAR_CORES), branch_weight, gate_weight)
    arrived = lax.all_gather(outgoing_block, "zh")
    total = arrived[:, :height].sum(axis=0)
    projected = from_everyone(total, NEAR_CORES).reshape(both.shape)

    entries = 2 * rank * width * lax.axis_size("tp")
    moments = (branch_first, gate_first, branch_second, gate_second)
    parts, squares = directions(projected, *moments)
    squares = from_everyone(squares, ("tp",))
    rows_new = new_rows(entries, squares, parts, far_factors, arrived)

    mine = from_everyone(rows_new, NEAR).reshape(*near, *rows_new.shape)
    other = swapped(mine)
    copies = place_mine(mine)
    (
        branch_step,
        gate_step,
        branch_new,
        gate_new,
        branch_first_new,
        gate_first_new,
        branch_second_new,
        gate_second_new,
    ) = results(
        entries,
        projected,
        moments,
        squares,
        parts,
        (branch_factor, gate_factor),
        (branch_weight, gate_weight),
    )
    branch_copy, gate_copy = [c.reshape(-1, width) for c in place_other(other, *copies)]
    return (
        branch_step,
        gate_step,
        branch_new,
        gate_new,
        branch_copy,
        gate_copy,
        branch_first_new,
        gate_first_new,
        branch_second_new,
        gate_second_new,
    )


def solution(mesh):
    finer = Mesh(
        mesh.devices.reshape(8, 2, 4, 2, mesh.shape["tp"]), ("zh", "zl", "x", "c", "tp")
    )
    sharded = P(FS, None)
    split = P(FS, "tp")
    kept = P(None, "tp")
    in_specs = (sharded, split, split, sharded, sharded, split, split, kept, kept, kept, kept)
    out_specs = (split, split, split, split, kept, kept, kept, kept, kept, kept)
    return jax.shard_map(body, mesh=finer, in_specs=in_specs, out_specs=out_specs, check_vma=False)
```

```python
import functools

import jax
import jax.numpy as jnp
from jax import lax
from jax.experimental import pallas as pl
from jax.experimental.pallas import tpu as pltpu
from jax.sharding import Mesh
from jax.sharding import PartitionSpec as P


FS = ("zh", "zl", "x", "c")
FAR = ("zh",)
Z = ("zh", "zl")
NEAR = ("zl", "x")
NEAR_CORES = ("zl", "x", "c")

first_decay = 0.8
second_decay = 0.9
learn_rate = 0.5


def size_of(axes):
    peers = 1
    for a in axes:
        peers *= lax.axis_size(a)
    return peers


def exchanged(blocks, axes):
    return lax.all_to_all(blocks, axes, split_axis=0, concat_axis=0, tiled=True)


def from_everyone(x, axes):
    return exchanged(jnp.broadcast_to(x, (size_of(axes), *x.shape)), axes)


def swapped(x):
    return lax.ppermute(x, "c", [(0, 1), (1, 0)])


def two_parts(x):
    high = lax.reduce_precision(x, 8, 7)
    return high.astype(jnp.bfloat16), (x - high).astype(jnp.bfloat16)


def projected_locally(rows, cotangent):
    high, low = two_parts(rows)
    rank = rows.shape[1]
    both = lax.dot_general(
        jnp.concatenate([high, low], axis=1),
        cotangent,
        (((0,), (0,)), ((), ())),
        preferred_element_type=jnp.float32,
    )
    return both[:rank] + both[rank:]


def moved_and_spread(projected, first, second):
    moved = first_decay * first + (1.0 - first_decay) * projected
    spread = second_decay * second + (1.0 - second_decay) * projected * projected
    return moved, spread


def part_of(projected, p):
    groups, _, height, width = projected.shape
    return projected[:, p].reshape(groups * height, width)


def direction_kernel(
    projected, branch_first, gate_first, branch_second, gate_second, parts, squares
):
    rank, width = branch_first.shape
    total = jnp.zeros((8, 128), jnp.float32)
    both = ((branch_first, branch_second), (gate_first, gate_second))
    for p, (first, second) in enumerate(both):
        moved, spread = moved_and_spread(part_of(projected, p), first[...], second[...])
        direction = moved / jnp.sqrt(spread)
        high = direction.astype(jnp.bfloat16)
        rest = direction - high.astype(jnp.float32)
        middle = rest.astype(jnp.bfloat16)
        low = (rest - middle.astype(jnp.float32)).astype(jnp.bfloat16)
        parts[p, :, :width] = high
        parts[p, :, width : 2 * width] = middle
        parts[p, :, 2 * width :] = low
        squared = direction * direction
        for column in range(0, width, 128):
            total += jnp.sum(
                squared[:, column : column + 128].reshape(rank // 8, 8, 128), axis=0
            )
    squares[...] = total


def scale_of(entries, squares):
    total = jnp.sum(jnp.sum(squares, axis=0), keepdims=True)
    return -learn_rate / jnp.sqrt(total / entries + 1e-06)


def times_parts(factor, parts):
    width = parts.shape[1] // 3
    out = jnp.dot(factor, parts, preferred_element_type=jnp.float32)
    return out[:, :width] + (out[:, width : 2 * width] + out[:, 2 * width :])


def rows_kernel(entries, squares, parts, factors, arrived, rows_new):
    near_z, _, far, block, _ = factors.shape
    rank = parts.shape[1]
    width = arrived.shape[3]
    x = lax.axis_index("x")
    minus_scale = scale_of(entries, squares[...])
    for z in range(near_z):
        for p in range(2):
            factor = factors[z, x, :, :, p * rank : (p + 1) * rank].reshape(far * block, rank)
            step = (minus_scale * times_parts(factor, parts[p])).reshape(far, block, width)
            weights = arrived[:, z, (p + 1) * block : (p + 2) * block, :]
            rows_new[z, :, :, p * width : (p + 1) * width] = (weights + step).astype(jnp.bfloat16)


def results_kernel(
    entries,
    projected,
    branch_first,
    gate_first,
    branch_second,
    gate_second,
    squares,
    parts,
    branch_factor,
    gate_factor,
    branch_weight,
    gate_weight,
    branch_step,
    gate_step,
    branch_new,
    gate_new,
    branch_first_new,
    gate_first_new,
    branch_second_new,
    gate_second_new,
):
    minus_scale = scale_of(entries, squares[...])
    both = (
        (branch_first, branch_second, branch_first_new, branch_second_new),
        (gate_first, gate_second, gate_first_new, gate_second_new),
    )
    for p, (first, second, first_new, second_new) in enumerate(both):
        moved, spread = moved_and_spread(part_of(projected, p), first[...], second[...])
        first_new[...] = moved
        second_new[...] = spread
    rows = (
        (branch_factor, branch_weight, branch_step, branch_new),
        (gate_factor, gate_weight, gate_step, gate_new),
    )
    for p, (factor, weight, step_out, new_out) in enumerate(rows):
        step = minus_scale * times_parts(factor[...], parts[p])
        step_out[...] = step
        new_out[...] = weight[...] + step


def outgoing_kernel(pieces, branch_weight, gate_weight, outgoing_block):
    height = pieces.shape[1]
    block = branch_weight.shape[0]
    outgoing_block[:height] = jnp.sum(pieces[...], axis=0)
    outgoing_block[height : height + block] = branch_weight[...]
    outgoing_block[height + block :] = gate_weight[...]


def factors_kernel(mine, other, factors):
    near_z, near_x, far, block, _ = mine.shape
    core = lax.axis_index("c")
    for f in range(far):
        for z in range(near_z):
            for x in range(near_x):
                row = ((f * near_z + z) * near_x + x) * 2 * block
                for source, place in ((mine, core), (other, 1 - core)):
                    rows = pl.ds(pl.multiple_of(row + place * block, block), block)
                    factors[rows, :] = source[z, x, f]


def placed(blocks, place, copies, done):
    near_x, near_z = blocks.shape[:2]
    width = copies[0].shape[-1]
    started = []
    for p, copy in enumerate(copies):
        for z in range(near_z):
            for x in range(near_x):
                started.append(
                    pltpu.make_async_copy(
                        blocks.at[x, z, :, :, pl.ds(p * width, width)],
                        copy.at[:, z, x, place],
                        done.at[len(started)],
                    )
                )
    for one in started:
        one.start()
    for one in started:
        one.wait()


def mine_kernel(mine, branch_copy, gate_copy, done):
    placed(mine, lax.axis_index("c"), (branch_copy, gate_copy), done)


def other_kernel(other, branch_in, gate_in, branch_copy, gate_copy, done):
    del branch_in, gate_in
    placed(other, 1 - lax.axis_index("c"), (branch_copy, gate_copy), done)


def whole():
    return pl.BlockSpec(memory_space=pltpu.VMEM)


def anywhere():
    return pl.BlockSpec(memory_space=pl.ANY)


def grant(mib):
    return pltpu.CompilerParams(vmem_limit_bytes=mib << 20)


def outgoing(pieces, branch_weight, gate_weight):
    height = pieces.shape[1] + 2 * branch_weight.shape[0]
    return pl.pallas_call(
        outgoing_kernel,
        out_shape=jax.ShapeDtypeStruct((height, pieces.shape[2]), jnp.float32),
        in_specs=[whole()] * 3,
        out_specs=whole(),
        compiler_params=grant(4),
        name="outgoing",
    )(pieces, branch_weight, gate_weight)


def whole_factors(mine, other):
    near_z, near_x, far, block, columns = mine.shape
    return pl.pallas_call(
        factors_kernel,
        out_shape=jax.ShapeDtypeStruct((2 * near_z * near_x * far * block, columns), mine.dtype),
        in_specs=[whole()] * 2,
        out_specs=whole(),
        compiler_params=grant(4),
        name="whole_factors",
    )(mine, other)


def copies_of(mine):
    near_x, near_z, far, block, columns = mine.shape
    copy = jax.ShapeDtypeStruct((far, near_z, near_x, 2, block, columns // 2), mine.dtype)
    return [copy, copy], [pltpu.SemaphoreType.DMA((2 * near_z * near_x,))]


def place_mine(mine):
    shapes, scratch = copies_of(mine)
    return pl.pallas_call(
        mine_kernel,
        out_shape=shapes,
        in_specs=[whole()],
        out_specs=[anywhere()] * 2,
        scratch_shapes=scratch,
        compiler_params=grant(4),
        cost_estimate=pl.CostEstimate(flops=1 << 20, bytes_accessed=1 << 21, transcendentals=0),
        name="place_mine",
    )(mine)


def place_other(other, branch_copy, gate_copy):
    shapes, scratch = copies_of(other)
    return pl.pallas_call(
        other_kernel,
        out_shape=shapes,
        in_specs=[whole(), anywhere(), anywhere()],
        out_specs=[anywhere()] * 2,
        scratch_shapes=scratch,
        input_output_aliases={1: 0, 2: 1},
        compiler_params=grant(4),
        name="place_other",
    )(other, branch_copy, gate_copy)


def directions(projected, branch_first, gate_first, branch_second, gate_second):
    rank, width = branch_first.shape
    return pl.pallas_call(
        direction_kernel,
        out_shape=[
            jax.ShapeDtypeStruct((2, rank, 3 * width), jnp.bfloat16),
            jax.ShapeDtypeStruct((8, 128), jnp.float32),
        ],
        in_specs=[whole()] * 5,
        out_specs=[whole()] * 2,
        compiler_params=grant(6),
        name="directions",
    )(projected, branch_first, gate_first, branch_second, gate_second)


def new_rows(entries, squares, parts, factors, arrived):
    near_z, _, far, block, _ = factors.shape
    columns = 2 * arrived.shape[3]
    return pl.pallas_call(
        functools.partial(rows_kernel, entries),
        out_shape=jax.ShapeDtypeStruct((near_z, far, block, columns), jnp.bfloat16),
        in_specs=[whole()] * 4,
        out_specs=whole(),
        compiler_params=grant(8),
        name="new_rows",
    )(squares, parts, factors, arrived)


def results(entries, projected, moments, squares, parts, factors, weights):
    rank, width = moments[0].shape
    block = weights[0].shape[0]
    row = jax.ShapeDtypeStruct((block, width), jnp.float32)
    moment = jax.ShapeDtypeStruct((rank, width), jnp.float32)
    return pl.pallas_call(
        functools.partial(results_kernel, entries),
        out_shape=[row] * 4 + [moment] * 4,
        in_specs=[whole()] * 11,
        out_specs=[whole()] * 8,
        compiler_params=grant(6),
        cost_estimate=pl.CostEstimate(flops=1 << 22, bytes_accessed=1 << 21, transcendentals=0),
        name="results",
    )(projected, *moments, squares, parts, *factors, *weights)


def body(
    layer_input,
    branch_cotangent,
    gate_cotangent,
    branch_factor,
    gate_factor,
    branch_weight,
    gate_weight,
    branch_first,
    gate_first,
    branch_second,
    gate_second,
):
    rank, width = branch_first.shape
    near = (lax.axis_size("zl"), lax.axis_size("x"))

    far_factors = from_everyone(jnp.concatenate([branch_factor, gate_factor], axis=1), FAR)
    near_factors = from_everyone(far_factors, NEAR).reshape(*near, *far_factors.shape)
    factors = whole_factors(near_factors, swapped(near_factors))

    rows = jnp.dot(layer_input, factors, preferred_element_type=jnp.float32)
    both = jnp.stack(
        [
            projected_locally(rows[:, :rank], branch_cotangent),
            projected_locally(rows[:, rank:], gate_cotangent),
        ]
    )
    pieces = both.reshape(size_of(NEAR_CORES), -1, width)
    height = pieces.shape[1]
    outgoing_block = outgoing(exchanged(pieces, NEAR_CORES), branch_weight, gate_weight)
    arrived = lax.all_gather(outgoing_block, Z).reshape(-1, near[0], *outgoing_block.shape)
    total = arrived[:, :, :height].sum(axis=0)
    projected = from_everyone(total, ("x", "c"))

    entries = 2 * rank * width * lax.axis_size("tp")
    moments = (branch_first, gate_first, branch_second, gate_second)
    parts, squares = directions(projected, *moments)
    squares = from_everyone(squares, ("tp",))
    rows_new = new_rows(entries, squares, parts, near_factors, arrived)

    mine = from_everyone(rows_new, ("x",))
    other = swapped(mine)
    copies = place_mine(mine)
    (
        branch_step,
        gate_step,
        branch_new,
        gate_new,
        branch_first_new,
        gate_first_new,
        branch_second_new,
        gate_second_new,
    ) = results(
        entries,
        projected,
        moments,
        squares,
        parts,
        (branch_factor, gate_factor),
        (branch_weight, gate_weight),
    )
    branch_copy, gate_copy = [c.reshape(-1, width) for c in place_other(other, *copies)]
    return (
        branch_step,
        gate_step,
        branch_new,
        gate_new,
        branch_copy,
        gate_copy,
        branch_first_new,
        gate_first_new,
        branch_second_new,
        gate_second_new,
    )


def solution(mesh):
    finer = Mesh(
        mesh.devices.reshape(8, 2, 4, 2, mesh.shape["tp"]), ("zh", "zl", "x", "c", "tp")
    )
    sharded = P(FS, None)
    split = P(FS, "tp")
    kept = P(None, "tp")
    in_specs = (sharded, split, split, sharded, sharded, split, split, kept, kept, kept, kept)
    out_specs = (split, split, split, split, kept, kept, kept, kept, kept, kept)
    return jax.shard_map(body, mesh=finer, in_specs=in_specs, out_specs=out_specs, check_vma=False)
```

```python
import functools

import jax
import jax.numpy as jnp
from jax import lax
from jax.experimental import pallas as pl
from jax.experimental.pallas import tpu as pltpu
from jax.sharding import Mesh
from jax.sharding import PartitionSpec as P


FS = ("zh", "zl", "x", "c")
FAR = ("zh",)
NEAR = ("zl", "x")
NEAR_CORES = ("zl", "x", "c")

first_decay = 0.8
second_decay = 0.9
learn_rate = 0.5


def size_of(axes):
    peers = 1
    for a in axes:
        peers *= lax.axis_size(a)
    return peers


def exchanged(blocks, axes):
    return lax.all_to_all(blocks, axes, split_axis=0, concat_axis=0, tiled=True)


def from_everyone(x, axes):
    return exchanged(jnp.broadcast_to(x, (size_of(axes), *x.shape)), axes)


def swapped(x):
    return lax.ppermute(x, "c", [(0, 1), (1, 0)])


def two_parts(x):
    high = lax.reduce_precision(x, 8, 7)
    return high.astype(jnp.bfloat16), (x - high).astype(jnp.bfloat16)


def projected_locally(rows, cotangent):
    high, low = two_parts(rows)
    rank = rows.shape[1]
    both = lax.dot_general(
        jnp.concatenate([high, low], axis=1),
        cotangent,
        (((0,), (0,)), ((), ())),
        preferred_element_type=jnp.float32,
    )
    return both[:rank] + both[rank:]


def moved_and_spread(projected, first, second):
    moved = first_decay * first + (1.0 - first_decay) * projected
    spread = second_decay * second + (1.0 - second_decay) * projected * projected
    return moved, spread


def direction_kernel(
    projected, branch_first, gate_first, branch_second, gate_second, parts, squares
):
    rank, width = branch_first.shape
    total = jnp.zeros((8, 128), jnp.float32)
    both = ((branch_first, branch_second), (gate_first, gate_second))
    for p, (first, second) in enumerate(both):
        moved, spread = moved_and_spread(projected[p], first[...], second[...])
        direction = moved / jnp.sqrt(spread)
        high = direction.astype(jnp.bfloat16)
        rest = direction - high.astype(jnp.float32)
        middle = rest.astype(jnp.bfloat16)
        low = (rest - middle.astype(jnp.float32)).astype(jnp.bfloat16)
        parts[p, :, :width] = high
        parts[p, :, width : 2 * width] = middle
        parts[p, :, 2 * width :] = low
        squared = direction * direction
        for column in range(0, width, 128):
            total += jnp.sum(
                squared[:, column : column + 128].reshape(rank // 8, 8, 128), axis=0
            )
    squares[...] = total


def scale_of(entries, squares):
    total = jnp.sum(jnp.sum(squares, axis=0), keepdims=True)
    return -learn_rate / jnp.sqrt(total / entries + 1e-06)


def times_parts(factor, parts):
    width = parts.shape[1] // 3
    out = jnp.dot(factor, parts, preferred_element_type=jnp.float32)
    return out[:, :width] + (out[:, width : 2 * width] + out[:, 2 * width :])


def rows_kernel(entries, squares, parts, factors, arrived, rows_new):
    far, block, _ = factors.shape
    rank = parts.shape[1]
    width = arrived.shape[2]
    minus_scale = scale_of(entries, squares[...])
    for p in range(2):
        factor = factors[:, :, p * rank : (p + 1) * rank].reshape(far * block, rank)
        step = (minus_scale * times_parts(factor, parts[p])).reshape(far, block, width)
        weights = arrived[:, (p + 1) * block : (p + 2) * block, :]
        rows_new[:, :, p * width : (p + 1) * width] = (weights + step).astype(jnp.bfloat16)


def results_kernel(
    entries,
    projected,
    branch_first,
    gate_first,
    branch_second,
    gate_second,
    squares,
    parts,
    branch_factor,
    gate_factor,
    branch_weight,
    gate_weight,
    branch_step,
    gate_step,
    branch_new,
    gate_new,
    branch_first_new,
    gate_first_new,
    branch_second_new,
    gate_second_new,
):
    minus_scale = scale_of(entries, squares[...])
    both = (
        (branch_first, branch_second, branch_first_new, branch_second_new),
        (gate_first, gate_second, gate_first_new, gate_second_new),
    )
    for p, (first, second, first_new, second_new) in enumerate(both):
        moved, spread = moved_and_spread(projected[p], first[...], second[...])
        first_new[...] = moved
        second_new[...] = spread
    rows = (
        (branch_factor, branch_weight, branch_step, branch_new),
        (gate_factor, gate_weight, gate_step, gate_new),
    )
    for p, (factor, weight, step_out, new_out) in enumerate(rows):
        step = minus_scale * times_parts(factor[...], parts[p])
        step_out[...] = step
        new_out[...] = weight[...] + step


def outgoing_kernel(pieces, branch_weight, gate_weight, blocks):
    height = pieces.shape[1]
    block = branch_weight.shape[0]
    piece = jnp.sum(pieces[...], axis=0)
    for peer in range(blocks.shape[0]):
        blocks[peer, :height] = piece
        blocks[peer, height : height + block] = branch_weight[...]
        blocks[peer, height + block :] = gate_weight[...]


def factors_kernel(mine, other, factors):
    near_z, near_x, far, block, _ = mine.shape
    core = lax.axis_index("c")
    for f in range(far):
        for z in range(near_z):
            for x in range(near_x):
                row = ((f * near_z + z) * near_x + x) * 2 * block
                for source, place in ((mine, core), (other, 1 - core)):
                    rows = pl.ds(pl.multiple_of(row + place * block, block), block)
                    factors[rows, :] = source[z, x, f]


def placed(blocks, place, copies, done):
    near_z, near_x = blocks.shape[:2]
    width = copies[0].shape[-1]
    started = []
    for p, copy in enumerate(copies):
        for z in range(near_z):
            for x in range(near_x):
                started.append(
                    pltpu.make_async_copy(
                        blocks.at[z, x, :, :, pl.ds(p * width, width)],
                        copy.at[:, z, x, place],
                        done.at[len(started)],
                    )
                )
    for one in started:
        one.start()
    for one in started:
        one.wait()


def mine_kernel(mine, branch_copy, gate_copy, done):
    placed(mine, lax.axis_index("c"), (branch_copy, gate_copy), done)


def other_kernel(other, branch_in, gate_in, branch_copy, gate_copy, done):
    del branch_in, gate_in
    placed(other, 1 - lax.axis_index("c"), (branch_copy, gate_copy), done)


def whole():
    return pl.BlockSpec(memory_space=pltpu.VMEM)


def anywhere():
    return pl.BlockSpec(memory_space=pl.ANY)


def grant(mib):
    return pltpu.CompilerParams(vmem_limit_bytes=mib << 20)


def outgoing(pieces, branch_weight, gate_weight, peers):
    height = pieces.shape[1] + 2 * branch_weight.shape[0]
    return pl.pallas_call(
        outgoing_kernel,
        out_shape=jax.ShapeDtypeStruct((peers, height, pieces.shape[2]), jnp.float32),
        in_specs=[whole()] * 3,
        out_specs=whole(),
        compiler_params=grant(4),
        name="outgoing",
    )(pieces, branch_weight, gate_weight)


def whole_factors(mine, other):
    near_z, near_x, far, block, columns = mine.shape
    return pl.pallas_call(
        factors_kernel,
        out_shape=jax.ShapeDtypeStruct((2 * near_z * near_x * far * block, columns), mine.dtype),
        in_specs=[whole()] * 2,
        out_specs=whole(),
        compiler_params=grant(4),
        name="whole_factors",
    )(mine, other)


def copies_of(mine):
    near_z, near_x, far, block, columns = mine.shape
    copy = jax.ShapeDtypeStruct((far, near_z, near_x, 2, block, columns // 2), mine.dtype)
    return [copy, copy], [pltpu.SemaphoreType.DMA((2 * near_z * near_x,))]


def place_mine(mine):
    shapes, scratch = copies_of(mine)
    return pl.pallas_call(
        mine_kernel,
        out_shape=shapes,
        in_specs=[whole()],
        out_specs=[anywhere()] * 2,
        scratch_shapes=scratch,
        compiler_params=grant(4),
        cost_estimate=pl.CostEstimate(flops=1 << 20, bytes_accessed=1 << 21, transcendentals=0),
        name="place_mine",
    )(mine)


def place_other(other, branch_copy, gate_copy):
    shapes, scratch = copies_of(other)
    return pl.pallas_call(
        other_kernel,
        out_shape=shapes,
        in_specs=[whole(), anywhere(), anywhere()],
        out_specs=[anywhere()] * 2,
        scratch_shapes=scratch,
        input_output_aliases={1: 0, 2: 1},
        compiler_params=grant(4),
        name="place_other",
    )(other, branch_copy, gate_copy)


def directions(projected, branch_first, gate_first, branch_second, gate_second):
    rank, width = branch_first.shape
    return pl.pallas_call(
        direction_kernel,
        out_shape=[
            jax.ShapeDtypeStruct((2, rank, 3 * width), jnp.bfloat16),
            jax.ShapeDtypeStruct((8, 128), jnp.float32),
        ],
        in_specs=[whole()] * 5,
        out_specs=[whole()] * 2,
        compiler_params=grant(6),
        name="directions",
    )(projected, branch_first, gate_first, branch_second, gate_second)


def new_rows(entries, squares, parts, factors, arrived):
    far, block, _ = factors.shape
    return pl.pallas_call(
        functools.partial(rows_kernel, entries),
        out_shape=jax.ShapeDtypeStruct((far, block, 2 * arrived.shape[2]), jnp.bfloat16),
        in_specs=[whole()] * 4,
        out_specs=whole(),
        compiler_params=grant(6),
        name="new_rows",
    )(squares, parts, factors, arrived)


def results(entries, projected, moments, squares, parts, factors, weights):
    rank, width = moments[0].shape
    block = weights[0].shape[0]
    row = jax.ShapeDtypeStruct((block, width), jnp.float32)
    moment = jax.ShapeDtypeStruct((rank, width), jnp.float32)
    return pl.pallas_call(
        functools.partial(results_kernel, entries),
        out_shape=[row] * 4 + [moment] * 4,
        in_specs=[whole()] * 11,
        out_specs=[whole()] * 8,
        compiler_params=grant(6),
        cost_estimate=pl.CostEstimate(flops=1 << 22, bytes_accessed=1 << 21, transcendentals=0),
        name="results",
    )(projected, *moments, squares, parts, *factors, *weights)


def body(
    layer_input,
    branch_cotangent,
    gate_cotangent,
    branch_factor,
    gate_factor,
    branch_weight,
    gate_weight,
    branch_first,
    gate_first,
    branch_second,
    gate_second,
):
    rank, width = branch_first.shape
    near = (lax.axis_size("zl"), lax.axis_size("x"))

    far_factors = from_everyone(jnp.concatenate([branch_factor, gate_factor], axis=1), FAR)
    near_factors = from_everyone(far_factors, NEAR).reshape(*near, *far_factors.shape)
    factors = whole_factors(near_factors, swapped(near_factors))

    rows = jnp.dot(layer_input, factors, preferred_element_type=jnp.float32)
    both = jnp.stack(
        [
            projected_locally(rows[:, :rank], branch_cotangent),
            projected_locally(rows[:, rank:], gate_cotangent),
        ]
    )
    pieces = both.reshape(size_of(NEAR_CORES), -1, width)
    height = pieces.shape[1]
    blocks = outgoing(
        exchanged(pieces, NEAR_CORES), branch_weight, gate_weight, size_of(FAR)
    )
    arrived = exchanged(blocks, FAR)
    total = arrived[:, :height].sum(axis=0)
    projected = from_everyone(total, NEAR_CORES).reshape(both.shape)

    entries = 2 * rank * width * lax.axis_size("tp")
    moments = (branch_first, gate_first, branch_second, gate_second)
    parts, squares = directions(projected, *moments)
    squares = from_everyone(squares, ("tp",))
    rows_new = new_rows(entries, squares, parts, far_factors, arrived)

    mine = from_everyone(rows_new, NEAR).reshape(*near, *rows_new.shape)
    other = swapped(mine)
    copies = place_mine(mine)
    (
        branch_step,
        gate_step,
        branch_new,
        gate_new,
        branch_first_new,
        gate_first_new,
        branch_second_new,
        gate_second_new,
    ) = results(
        entries,
        projected,
        moments,
        squares,
        parts,
        (branch_factor, gate_factor),
        (branch_weight, gate_weight),
    )
    branch_copy, gate_copy = [c.reshape(-1, width) for c in place_other(other, *copies)]
    return (
        branch_step,
        gate_step,
        branch_new,
        gate_new,
        branch_copy,
        gate_copy,
        branch_first_new,
        gate_first_new,
        branch_second_new,
        gate_second_new,
    )


def solution(mesh):
    finer = Mesh(
        mesh.devices.reshape(8, 2, 4, 2, mesh.shape["tp"]), ("zh", "zl", "x", "c", "tp")
    )
    sharded = P(FS, None)
    split = P(FS, "tp")
    kept = P(None, "tp")
    in_specs = (sharded, split, split, sharded, sharded, split, split, kept, kept, kept, kept)
    out_specs = (split, split, split, split, kept, kept, kept, kept, kept, kept)
    return jax.shard_map(body, mesh=finer, in_specs=in_specs, out_specs=out_specs, check_vma=False)
```

```python
import functools

import jax
import jax.numpy as jnp
from jax import lax
from jax.experimental import pallas as pl
from jax.experimental.pallas import tpu as pltpu
from jax.sharding import Mesh
from jax.sharding import PartitionSpec as P


FS = ("zh", "zm", "zl", "x", "c")
FAR = ("zh", "zm")
NEAR = ("zl", "x")
NEAR_CORES = ("zm", "zl", "x", "c")

first_decay = 0.8
second_decay = 0.9
learn_rate = 0.5


def size_of(axes):
    peers = 1
    for a in axes:
        peers *= lax.axis_size(a)
    return peers


def exchanged(blocks, axes):
    return lax.all_to_all(blocks, axes, split_axis=0, concat_axis=0, tiled=True)


def from_everyone(x, axes):
    return exchanged(jnp.broadcast_to(x, (size_of(axes), *x.shape)), axes)


def swapped(x, axis="c"):
    return lax.ppermute(x, axis, [(0, 1), (1, 0)])


def two_parts(x):
    high = lax.reduce_precision(x, 8, 7)
    return high.astype(jnp.bfloat16), (x - high).astype(jnp.bfloat16)


def projected_locally(rows, cotangent):
    high, low = two_parts(rows)
    rank = rows.shape[1]
    both = lax.dot_general(
        jnp.concatenate([high, low], axis=1),
        cotangent,
        (((0,), (0,)), ((), ())),
        preferred_element_type=jnp.float32,
    )
    return both[:rank] + both[rank:]


def moved_and_spread(projected, first, second):
    moved = first_decay * first + (1.0 - first_decay) * projected
    spread = second_decay * second + (1.0 - second_decay) * projected * projected
    return moved, spread


def direction_kernel(
    projected, branch_first, gate_first, branch_second, gate_second, parts, squares
):
    rank, width = branch_first.shape
    total = jnp.zeros((8, 128), jnp.float32)
    both = ((branch_first, branch_second), (gate_first, gate_second))
    for p, (first, second) in enumerate(both):
        moved, spread = moved_and_spread(projected[p], first[...], second[...])
        direction = moved / jnp.sqrt(spread)
        high = direction.astype(jnp.bfloat16)
        rest = direction - high.astype(jnp.float32)
        middle = rest.astype(jnp.bfloat16)
        low = (rest - middle.astype(jnp.float32)).astype(jnp.bfloat16)
        parts[p, :, :width] = high
        parts[p, :, width : 2 * width] = middle
        parts[p, :, 2 * width :] = low
        squared = direction * direction
        for column in range(0, width, 128):
            total += jnp.sum(
                squared[:, column : column + 128].reshape(rank // 8, 8, 128), axis=0
            )
    squares[...] = total


def scale_of(entries, squares):
    total = jnp.sum(jnp.sum(squares, axis=0), keepdims=True)
    return -learn_rate / jnp.sqrt(total / entries + 1e-06)


def times_parts(factor, parts):
    width = parts.shape[1] // 3
    out = jnp.dot(factor, parts, preferred_element_type=jnp.float32)
    return out[:, :width] + (out[:, width : 2 * width] + out[:, 2 * width :])


def rows_kernel(entries, squares, parts, factors, arrived, other, rows_new):
    _, block, _ = factors.shape
    rank = parts.shape[1]
    far, _, width = arrived.shape
    height = arrived.shape[1] - 2 * block
    me = lax.axis_index("zm")
    minus_scale = scale_of(entries, squares[...])
    for source, place in ((arrived, me), (other, 1 - me)):
        for p in range(2):
            columns = slice(p * width, (p + 1) * width)
            ranks = slice(p * rank, (p + 1) * rank)
            factor = jnp.concatenate([factors[2 * f + place, :, ranks] for f in range(far)], axis=0)
            step = minus_scale * times_parts(factor, parts[p])
            for f in range(far):
                weights = source[f, height + p * block : height + (p + 1) * block, :]
                new = weights + step[f * block : (f + 1) * block]
                rows_new[2 * f + place, :, columns] = new.astype(jnp.bfloat16)


def results_kernel(
    entries,
    projected,
    branch_first,
    gate_first,
    branch_second,
    gate_second,
    squares,
    parts,
    branch_factor,
    gate_factor,
    branch_weight,
    gate_weight,
    branch_step,
    gate_step,
    branch_new,
    gate_new,
    branch_first_new,
    gate_first_new,
    branch_second_new,
    gate_second_new,
):
    minus_scale = scale_of(entries, squares[...])
    both = (
        (branch_first, branch_second, branch_first_new, branch_second_new),
        (gate_first, gate_second, gate_first_new, gate_second_new),
    )
    for p, (first, second, first_new, second_new) in enumerate(both):
        moved, spread = moved_and_spread(projected[p], first[...], second[...])
        first_new[...] = moved
        second_new[...] = spread
    rows = (
        (branch_factor, branch_weight, branch_step, branch_new),
        (gate_factor, gate_weight, gate_step, gate_new),
    )
    for p, (factor, weight, step_out, new_out) in enumerate(rows):
        step = minus_scale * times_parts(factor[...], parts[p])
        step_out[...] = step
        new_out[...] = weight[...] + step


def outgoing_kernel(pieces, branch_weight, gate_weight, blocks):
    height = pieces.shape[1]
    block = branch_weight.shape[0]
    piece = jnp.sum(pieces[...], axis=0)
    for peer in range(blocks.shape[0]):
        blocks[peer, :height] = piece
        blocks[peer, height : height + block] = branch_weight[...]
        blocks[peer, height + block :] = gate_weight[...]


def factors_kernel(mine, other, factors):
    near_z, near_x, far, block, _ = mine.shape
    core = lax.axis_index("c")
    for f in range(far):
        for z in range(near_z):
            for x in range(near_x):
                row = ((f * near_z + z) * near_x + x) * 2 * block
                for source, place in ((mine, core), (other, 1 - core)):
                    rows = pl.ds(pl.multiple_of(row + place * block, block), block)
                    factors[rows, :] = source[z, x, f]


def placed(blocks, place, copies, done):
    near_z, near_x = blocks.shape[:2]
    width = copies[0].shape[-1]
    started = []
    for p, copy in enumerate(copies):
        for z in range(near_z):
            for x in range(near_x):
                started.append(
                    pltpu.make_async_copy(
                        blocks.at[z, x, :, :, pl.ds(p * width, width)],
                        copy.at[:, z, x, place],
                        done.at[len(started)],
                    )
                )
    for one in started:
        one.start()
    for one in started:
        one.wait()


def mine_kernel(mine, branch_copy, gate_copy, done):
    placed(mine, lax.axis_index("c"), (branch_copy, gate_copy), done)


def other_kernel(other, branch_in, gate_in, branch_copy, gate_copy, done):
    del branch_in, gate_in
    placed(other, 1 - lax.axis_index("c"), (branch_copy, gate_copy), done)


def whole():
    return pl.BlockSpec(memory_space=pltpu.VMEM)


def anywhere():
    return pl.BlockSpec(memory_space=pl.ANY)


def grant(mib):
    return pltpu.CompilerParams(vmem_limit_bytes=mib << 20)


def outgoing(pieces, branch_weight, gate_weight, peers):
    height = pieces.shape[1] + 2 * branch_weight.shape[0]
    return pl.pallas_call(
        outgoing_kernel,
        out_shape=jax.ShapeDtypeStruct((peers, height, pieces.shape[2]), jnp.float32),
        in_specs=[whole()] * 3,
        out_specs=whole(),
        compiler_params=grant(4),
        name="outgoing",
    )(pieces, branch_weight, gate_weight)


def whole_factors(mine, other):
    near_z, near_x, far, block, columns = mine.shape
    return pl.pallas_call(
        factors_kernel,
        out_shape=jax.ShapeDtypeStruct((2 * near_z * near_x * far * block, columns), mine.dtype),
        in_specs=[whole()] * 2,
        out_specs=whole(),
        compiler_params=grant(4),
        name="whole_factors",
    )(mine, other)


def copies_of(mine):
    near_z, near_x, far, block, columns = mine.shape
    copy = jax.ShapeDtypeStruct((far, near_z, near_x, 2, block, columns // 2), mine.dtype)
    return [copy, copy], [pltpu.SemaphoreType.DMA((2 * near_z * near_x,))]


def place_mine(mine):
    shapes, scratch = copies_of(mine)
    return pl.pallas_call(
        mine_kernel,
        out_shape=shapes,
        in_specs=[whole()],
        out_specs=[anywhere()] * 2,
        scratch_shapes=scratch,
        compiler_params=grant(4),
        cost_estimate=pl.CostEstimate(flops=1 << 20, bytes_accessed=1 << 21, transcendentals=0),
        name="place_mine",
    )(mine)


def place_other(other, branch_copy, gate_copy):
    shapes, scratch = copies_of(other)
    return pl.pallas_call(
        other_kernel,
        out_shape=shapes,
        in_specs=[whole(), anywhere(), anywhere()],
        out_specs=[anywhere()] * 2,
        scratch_shapes=scratch,
        input_output_aliases={1: 0, 2: 1},
        compiler_params=grant(4),
        name="place_other",
    )(other, branch_copy, gate_copy)


def directions(projected, branch_first, gate_first, branch_second, gate_second):
    rank, width = branch_first.shape
    return pl.pallas_call(
        direction_kernel,
        out_shape=[
            jax.ShapeDtypeStruct((2, rank, 3 * width), jnp.bfloat16),
            jax.ShapeDtypeStruct((8, 128), jnp.float32),
        ],
        in_specs=[whole()] * 5,
        out_specs=[whole()] * 2,
        compiler_params=grant(6),
        name="directions",
    )(projected, branch_first, gate_first, branch_second, gate_second)


def new_rows(entries, squares, parts, factors, arrived, other):
    far, block, _ = factors.shape
    return pl.pallas_call(
        functools.partial(rows_kernel, entries),
        out_shape=jax.ShapeDtypeStruct((far, block, 2 * arrived.shape[2]), jnp.bfloat16),
        in_specs=[whole()] * 5,
        out_specs=whole(),
        compiler_params=grant(6),
        name="new_rows",
    )(squares, parts, factors, arrived, other)


def results(entries, projected, moments, squares, parts, factors, weights):
    rank, width = moments[0].shape
    block = weights[0].shape[0]
    row = jax.ShapeDtypeStruct((block, width), jnp.float32)
    moment = jax.ShapeDtypeStruct((rank, width), jnp.float32)
    return pl.pallas_call(
        functools.partial(results_kernel, entries),
        out_shape=[row] * 4 + [moment] * 4,
        in_specs=[whole()] * 11,
        out_specs=[whole()] * 8,
        compiler_params=grant(6),
        cost_estimate=pl.CostEstimate(flops=1 << 22, bytes_accessed=1 << 21, transcendentals=0),
        name="results",
    )(projected, *moments, squares, parts, *factors, *weights)


def body(
    layer_input,
    branch_cotangent,
    gate_cotangent,
    branch_factor,
    gate_factor,
    branch_weight,
    gate_weight,
    branch_first,
    gate_first,
    branch_second,
    gate_second,
):
    rank, width = branch_first.shape
    near = (lax.axis_size("zl"), lax.axis_size("x"))

    far_factors = from_everyone(jnp.concatenate([branch_factor, gate_factor], axis=1), FAR)
    near_factors = from_everyone(far_factors, NEAR).reshape(*near, *far_factors.shape)
    factors = whole_factors(near_factors, swapped(near_factors))

    rows = jnp.dot(layer_input, factors, preferred_element_type=jnp.float32)
    both = jnp.stack(
        [
            projected_locally(rows[:, :rank], branch_cotangent),
            projected_locally(rows[:, rank:], gate_cotangent),
        ]
    )
    pieces = both.reshape(size_of(NEAR_CORES), -1, width)
    height = pieces.shape[1]
    blocks = outgoing(
        exchanged(pieces, NEAR_CORES), branch_weight, gate_weight, lax.axis_size("zh")
    )
    arrived = exchanged(blocks, ("zh",))
    total = arrived[:, :height].sum(axis=0)
    projected = from_everyone(total, NEAR_CORES).reshape(both.shape)
    other_arrived = swapped(arrived, "zm")

    entries = 2 * rank * width * lax.axis_size("tp")
    moments = (branch_first, gate_first, branch_second, gate_second)
    parts, squares = directions(projected, *moments)
    squares = from_everyone(squares, ("tp",))
    rows_new = new_rows(entries, squares, parts, far_factors, arrived, other_arrived)

    mine = from_everyone(rows_new, NEAR).reshape(*near, *rows_new.shape)
    other = swapped(mine)
    copies = place_mine(mine)
    (
        branch_step,
        gate_step,
        branch_new,
        gate_new,
        branch_first_new,
        gate_first_new,
        branch_second_new,
        gate_second_new,
    ) = results(
        entries,
        projected,
        moments,
        squares,
        parts,
        (branch_factor, gate_factor),
        (branch_weight, gate_weight),
    )
    branch_copy, gate_copy = [c.reshape(-1, width) for c in place_other(other, *copies)]
    return (
        branch_step,
        gate_step,
        branch_new,
        gate_new,
        branch_copy,
        gate_copy,
        branch_first_new,
        gate_first_new,
        branch_second_new,
        gate_second_new,
    )


def solution(mesh):
    finer = Mesh(
        mesh.devices.reshape(4, 2, 2, 4, 2, mesh.shape["tp"]),
        ("zh", "zm", "zl", "x", "c", "tp"),
    )
    sharded = P(FS, None)
    split = P(FS, "tp")
    kept = P(None, "tp")
    in_specs = (sharded, split, split, sharded, sharded, split, split, kept, kept, kept, kept)
    out_specs = (split, split, split, split, kept, kept, kept, kept, kept, kept)
    return jax.shard_map(body, mesh=finer, in_specs=in_specs, out_specs=out_specs, check_vma=False)
```

```python
import functools

import jax
import jax.numpy as jnp
from jax import lax
from jax.experimental import pallas as pl
from jax.experimental.pallas import tpu as pltpu
from jax.sharding import Mesh
from jax.sharding import PartitionSpec as P


FS = ("zh", "zm", "zl", "x", "c")
FAR = ("zh", "zm")
NEAR = ("zl", "x")
NEAR_CORES = ("zl", "x", "c")

first_decay = 0.8
second_decay = 0.9
learn_rate = 0.5


def size_of(axes):
    peers = 1
    for a in axes:
        peers *= lax.axis_size(a)
    return peers


def exchanged(blocks, axes):
    return lax.all_to_all(blocks, axes, split_axis=0, concat_axis=0, tiled=True)


def from_everyone(x, axes):
    return exchanged(jnp.broadcast_to(x, (size_of(axes), *x.shape)), axes)


def swapped(x, axis="c"):
    return lax.ppermute(x, axis, [(0, 1), (1, 0)])


def two_parts(x):
    high = lax.reduce_precision(x, 8, 7)
    return high.astype(jnp.bfloat16), (x - high).astype(jnp.bfloat16)


def projected_locally(rows, cotangent):
    high, low = two_parts(rows)
    rank = rows.shape[1]
    both = lax.dot_general(
        jnp.concatenate([high, low], axis=1),
        cotangent,
        (((0,), (0,)), ((), ())),
        preferred_element_type=jnp.float32,
    )
    return both[:rank] + both[rank:]


def moved_and_spread(projected, first, second):
    moved = first_decay * first + (1.0 - first_decay) * projected
    spread = second_decay * second + (1.0 - second_decay) * projected * projected
    return moved, spread


def direction_kernel(
    projected, branch_first, gate_first, branch_second, gate_second, parts, squares
):
    rank, width = branch_first.shape
    total = jnp.zeros((8, 128), jnp.float32)
    both = ((branch_first, branch_second), (gate_first, gate_second))
    for p, (first, second) in enumerate(both):
        moved, spread = moved_and_spread(projected[p], first[...], second[...])
        direction = moved / jnp.sqrt(spread)
        high = direction.astype(jnp.bfloat16)
        rest = direction - high.astype(jnp.float32)
        middle = rest.astype(jnp.bfloat16)
        low = (rest - middle.astype(jnp.float32)).astype(jnp.bfloat16)
        parts[p, :, :width] = high
        parts[p, :, width : 2 * width] = middle
        parts[p, :, 2 * width :] = low
        squared = direction * direction
        for column in range(0, width, 128):
            total += jnp.sum(
                squared[:, column : column + 128].reshape(rank // 8, 8, 128), axis=0
            )
    squares[...] = total


def scale_of(entries, squares):
    total = jnp.sum(jnp.sum(squares, axis=0), keepdims=True)
    return -learn_rate / jnp.sqrt(total / entries + 1e-06)


def times_parts(factor, parts):
    width = parts.shape[1] // 3
    out = jnp.dot(factor, parts, preferred_element_type=jnp.float32)
    return out[:, :width] + (out[:, width : 2 * width] + out[:, 2 * width :])


def rows_kernel(entries, squares, parts, factors, mine, other, rows_new):
    _, block, _ = factors.shape
    rank = parts.shape[1]
    far, _, width = mine.shape
    me = lax.axis_index("zm")
    minus_scale = scale_of(entries, squares[...])
    for source, place in ((mine, me), (other, 1 - me)):
        for p in range(2):
            columns = slice(p * width, (p + 1) * width)
            ranks = slice(p * rank, (p + 1) * rank)
            factor = jnp.concatenate([factors[2 * f + place, :, ranks] for f in range(far)], axis=0)
            step = minus_scale * times_parts(factor, parts[p])
            for f in range(far):
                weights = source[f, p * block : (p + 1) * block, :]
                new = weights + step[f * block : (f + 1) * block]
                rows_new[2 * f + place, :, columns] = new.astype(jnp.bfloat16)


def results_kernel(
    entries,
    projected,
    branch_first,
    gate_first,
    branch_second,
    gate_second,
    squares,
    parts,
    branch_factor,
    gate_factor,
    branch_weight,
    gate_weight,
    branch_step,
    gate_step,
    branch_new,
    gate_new,
    branch_first_new,
    gate_first_new,
    branch_second_new,
    gate_second_new,
):
    minus_scale = scale_of(entries, squares[...])
    both = (
        (branch_first, branch_second, branch_first_new, branch_second_new),
        (gate_first, gate_second, gate_first_new, gate_second_new),
    )
    for p, (first, second, first_new, second_new) in enumerate(both):
        moved, spread = moved_and_spread(projected[p], first[...], second[...])
        first_new[...] = moved
        second_new[...] = spread
    rows = (
        (branch_factor, branch_weight, branch_step, branch_new),
        (gate_factor, gate_weight, gate_step, gate_new),
    )
    for p, (factor, weight, step_out, new_out) in enumerate(rows):
        step = minus_scale * times_parts(factor[...], parts[p])
        step_out[...] = step
        new_out[...] = weight[...] + step


def outgoing_kernel(pieces, branch_weight, gate_weight, blocks):
    height = pieces.shape[1]
    block = branch_weight.shape[0]
    piece = jnp.sum(pieces[...], axis=0)
    for peer in range(blocks.shape[0]):
        blocks[peer, :height] = piece
        blocks[peer, height : height + block] = branch_weight[...]
        blocks[peer, height + block :] = gate_weight[...]


def factors_kernel(mine, other, factors):
    near_z, near_x, far, block, _ = mine.shape
    core = lax.axis_index("c")
    for f in range(far):
        for z in range(near_z):
            for x in range(near_x):
                row = ((f * near_z + z) * near_x + x) * 2 * block
                for source, place in ((mine, core), (other, 1 - core)):
                    rows = pl.ds(pl.multiple_of(row + place * block, block), block)
                    factors[rows, :] = source[z, x, f]


def placed(blocks, place, copies, done):
    near_z, near_x = blocks.shape[:2]
    width = copies[0].shape[-1]
    started = []
    for p, copy in enumerate(copies):
        for z in range(near_z):
            for x in range(near_x):
                started.append(
                    pltpu.make_async_copy(
                        blocks.at[z, x, :, :, pl.ds(p * width, width)],
                        copy.at[:, z, x, place],
                        done.at[len(started)],
                    )
                )
    for one in started:
        one.start()
    for one in started:
        one.wait()


def mine_kernel(mine, branch_copy, gate_copy, done):
    placed(mine, lax.axis_index("c"), (branch_copy, gate_copy), done)


def other_kernel(other, branch_in, gate_in, branch_copy, gate_copy, done):
    del branch_in, gate_in
    placed(other, 1 - lax.axis_index("c"), (branch_copy, gate_copy), done)


def whole():
    return pl.BlockSpec(memory_space=pltpu.VMEM)


def anywhere():
    return pl.BlockSpec(memory_space=pl.ANY)


def grant(mib):
    return pltpu.CompilerParams(vmem_limit_bytes=mib << 20)


def outgoing(pieces, branch_weight, gate_weight, peers):
    height = pieces.shape[1] + 2 * branch_weight.shape[0]
    return pl.pallas_call(
        outgoing_kernel,
        out_shape=jax.ShapeDtypeStruct((peers, height, pieces.shape[2]), jnp.float32),
        in_specs=[whole()] * 3,
        out_specs=whole(),
        compiler_params=grant(4),
        name="outgoing",
    )(pieces, branch_weight, gate_weight)


def whole_factors(mine, other):
    near_z, near_x, far, block, columns = mine.shape
    return pl.pallas_call(
        factors_kernel,
        out_shape=jax.ShapeDtypeStruct((2 * near_z * near_x * far * block, columns), mine.dtype),
        in_specs=[whole()] * 2,
        out_specs=whole(),
        compiler_params=grant(4),
        name="whole_factors",
    )(mine, other)


def copies_of(mine):
    near_z, near_x, far, block, columns = mine.shape
    copy = jax.ShapeDtypeStruct((far, near_z, near_x, 2, block, columns // 2), mine.dtype)
    return [copy, copy], [pltpu.SemaphoreType.DMA((2 * near_z * near_x,))]


def place_mine(mine):
    shapes, scratch = copies_of(mine)
    return pl.pallas_call(
        mine_kernel,
        out_shape=shapes,
        in_specs=[whole()],
        out_specs=[anywhere()] * 2,
        scratch_shapes=scratch,
        compiler_params=grant(4),
        cost_estimate=pl.CostEstimate(flops=1 << 20, bytes_accessed=1 << 21, transcendentals=0),
        name="place_mine",
    )(mine)


def place_other(other, branch_copy, gate_copy):
    shapes, scratch = copies_of(other)
    return pl.pallas_call(
        other_kernel,
        out_shape=shapes,
        in_specs=[whole(), anywhere(), anywhere()],
        out_specs=[anywhere()] * 2,
        scratch_shapes=scratch,
        input_output_aliases={1: 0, 2: 1},
        compiler_params=grant(4),
        name="place_other",
    )(other, branch_copy, gate_copy)


def directions(projected, branch_first, gate_first, branch_second, gate_second):
    rank, width = branch_first.shape
    return pl.pallas_call(
        direction_kernel,
        out_shape=[
            jax.ShapeDtypeStruct((2, rank, 3 * width), jnp.bfloat16),
            jax.ShapeDtypeStruct((8, 128), jnp.float32),
        ],
        in_specs=[whole()] * 5,
        out_specs=[whole()] * 2,
        compiler_params=grant(6),
        name="directions",
    )(projected, branch_first, gate_first, branch_second, gate_second)


def new_rows(entries, squares, parts, factors, mine, other):
    far, block, _ = factors.shape
    return pl.pallas_call(
        functools.partial(rows_kernel, entries),
        out_shape=jax.ShapeDtypeStruct((far, block, 2 * mine.shape[2]), jnp.bfloat16),
        in_specs=[whole()] * 5,
        out_specs=whole(),
        compiler_params=grant(6),
        name="new_rows",
    )(squares, parts, factors, mine, other)


def results(entries, projected, moments, squares, parts, factors, weights):
    rank, width = moments[0].shape
    block = weights[0].shape[0]
    row = jax.ShapeDtypeStruct((block, width), jnp.float32)
    moment = jax.ShapeDtypeStruct((rank, width), jnp.float32)
    return pl.pallas_call(
        functools.partial(results_kernel, entries),
        out_shape=[row] * 4 + [moment] * 4,
        in_specs=[whole()] * 11,
        out_specs=[whole()] * 8,
        compiler_params=grant(6),
        cost_estimate=pl.CostEstimate(flops=1 << 22, bytes_accessed=1 << 21, transcendentals=0),
        name="results",
    )(projected, *moments, squares, parts, *factors, *weights)


def body(
    layer_input,
    branch_cotangent,
    gate_cotangent,
    branch_factor,
    gate_factor,
    branch_weight,
    gate_weight,
    branch_first,
    gate_first,
    branch_second,
    gate_second,
):
    rank, width = branch_first.shape
    near = (lax.axis_size("zl"), lax.axis_size("x"))

    far_factors = from_everyone(jnp.concatenate([branch_factor, gate_factor], axis=1), FAR)
    near_factors = from_everyone(far_factors, NEAR).reshape(*near, *far_factors.shape)
    factors = whole_factors(near_factors, swapped(near_factors))

    rows = jnp.dot(layer_input, factors, preferred_element_type=jnp.float32)
    both = jnp.stack(
        [
            projected_locally(rows[:, :rank], branch_cotangent),
            projected_locally(rows[:, rank:], gate_cotangent),
        ]
    )
    pieces = both.reshape(size_of(NEAR_CORES), -1, width)
    height = pieces.shape[1]
    blocks = outgoing(
        exchanged(pieces, NEAR_CORES), branch_weight, gate_weight, lax.axis_size("zh")
    )
    arrived = exchanged(blocks, ("zh",))
    partial = arrived[:, :height].sum(axis=0)
    weights = arrived[:, height:]
    other_partial = swapped(partial, "zm")
    other_weights = swapped(weights, "zm")
    projected = from_everyone(partial + other_partial, NEAR_CORES).reshape(both.shape)

    entries = 2 * rank * width * lax.axis_size("tp")
    moments = (branch_first, gate_first, branch_second, gate_second)
    parts, squares = directions(projected, *moments)
    squares = from_everyone(squares, ("tp",))
    rows_new = new_rows(entries, squares, parts, far_factors, weights, other_weights)

    mine = from_everyone(rows_new, NEAR).reshape(*near, *rows_new.shape)
    other = swapped(mine)
    copies = place_mine(mine)
    (
        branch_step,
        gate_step,
        branch_new,
        gate_new,
        branch_first_new,
        gate_first_new,
        branch_second_new,
        gate_second_new,
    ) = results(
        entries,
        projected,
        moments,
        squares,
        parts,
        (branch_factor, gate_factor),
        (branch_weight, gate_weight),
    )
    branch_copy, gate_copy = [c.reshape(-1, width) for c in place_other(other, *copies)]
    return (
        branch_step,
        gate_step,
        branch_new,
        gate_new,
        branch_copy,
        gate_copy,
        branch_first_new,
        gate_first_new,
        branch_second_new,
        gate_second_new,
    )


def solution(mesh):
    finer = Mesh(
        mesh.devices.reshape(4, 2, 2, 4, 2, mesh.shape["tp"]),
        ("zh", "zm", "zl", "x", "c", "tp"),
    )
    sharded = P(FS, None)
    split = P(FS, "tp")
    kept = P(None, "tp")
    in_specs = (sharded, split, split, sharded, sharded, split, split, kept, kept, kept, kept)
    out_specs = (split, split, split, split, kept, kept, kept, kept, kept, kept)
    return jax.shard_map(body, mesh=finer, in_specs=in_specs, out_specs=out_specs, check_vma=False)
```

```python
import functools

import jax
import jax.numpy as jnp
from jax import lax
from jax.experimental import pallas as pl
from jax.experimental.pallas import tpu as pltpu
from jax.sharding import Mesh
from jax.sharding import PartitionSpec as P


FS = ("zh", "zm", "zl", "x", "c")
FAR = ("zh", "zm")
NEAR = ("zl", "x")
NEAR_CORES = ("zl", "x", "c")

first_decay = 0.8
second_decay = 0.9
learn_rate = 0.5


def size_of(axes):
    peers = 1
    for a in axes:
        peers *= lax.axis_size(a)
    return peers


def exchanged(blocks, axes):
    return lax.all_to_all(blocks, axes, split_axis=0, concat_axis=0, tiled=True)


def from_everyone(x, axes):
    return exchanged(jnp.broadcast_to(x, (size_of(axes), *x.shape)), axes)


def swapped(x, axis="c"):
    return lax.ppermute(x, axis, [(0, 1), (1, 0)])


def two_parts(x):
    high = lax.reduce_precision(x, 8, 7)
    return high.astype(jnp.bfloat16), (x - high).astype(jnp.bfloat16)


def projected_locally(rows, cotangent):
    high, low = two_parts(rows)
    rank = rows.shape[1]
    both = lax.dot_general(
        jnp.concatenate([high, low], axis=1),
        cotangent,
        (((0,), (0,)), ((), ())),
        preferred_element_type=jnp.float32,
    )
    return both[:rank] + both[rank:]


def moved_and_spread(projected, first, second):
    moved = first_decay * first + (1.0 - first_decay) * projected
    spread = second_decay * second + (1.0 - second_decay) * projected * projected
    return moved, spread


def direction_kernel(
    projected, branch_first, gate_first, branch_second, gate_second, parts, squares
):
    rank, width = branch_first.shape
    total = jnp.zeros((8, 128), jnp.float32)
    both = ((branch_first, branch_second), (gate_first, gate_second))
    for p, (first, second) in enumerate(both):
        moved, spread = moved_and_spread(projected[p], first[...], second[...])
        direction = moved / jnp.sqrt(spread)
        high = direction.astype(jnp.bfloat16)
        rest = direction - high.astype(jnp.float32)
        middle = rest.astype(jnp.bfloat16)
        low = (rest - middle.astype(jnp.float32)).astype(jnp.bfloat16)
        parts[p, :, :width] = high
        parts[p, :, width : 2 * width] = middle
        parts[p, :, 2 * width :] = low
        squared = direction * direction
        for column in range(0, width, 128):
            total += jnp.sum(
                squared[:, column : column + 128].reshape(rank // 8, 8, 128), axis=0
            )
    squares[...] = total


def scale_of(entries, squares):
    total = jnp.sum(jnp.sum(squares, axis=0), keepdims=True)
    return -learn_rate / jnp.sqrt(total / entries + 1e-06)


def times_parts(factor, parts):
    width = parts.shape[1] // 3
    out = jnp.dot(factor, parts, preferred_element_type=jnp.float32)
    return out[:, :width] + (out[:, width : 2 * width] + out[:, 2 * width :])


def rows_kernel(entries, squares, parts, factors, mine, other, rows_new):
    _, block, _ = factors.shape
    rank = parts.shape[1]
    far, _, width = mine.shape
    me = lax.axis_index("zm")
    minus_scale = scale_of(entries, squares[...])
    for source, place in ((mine, me), (other, 1 - me)):
        for p in range(2):
            columns = slice(p * width, (p + 1) * width)
            ranks = slice(p * rank, (p + 1) * rank)
            factor = jnp.concatenate([factors[2 * f + place, :, ranks] for f in range(far)], axis=0)
            step = minus_scale * times_parts(factor, parts[p])
            for f in range(far):
                weights = source[f, p * block : (p + 1) * block, :]
                new = weights + step[f * block : (f + 1) * block]
                for peer in range(rows_new.shape[0]):
                    rows_new[peer, 2 * f + place, :, columns] = new.astype(jnp.bfloat16)


def results_kernel(
    entries,
    projected,
    branch_first,
    gate_first,
    branch_second,
    gate_second,
    squares,
    parts,
    branch_factor,
    gate_factor,
    branch_weight,
    gate_weight,
    branch_step,
    gate_step,
    branch_new,
    gate_new,
    branch_first_new,
    gate_first_new,
    branch_second_new,
    gate_second_new,
):
    minus_scale = scale_of(entries, squares[...])
    both = (
        (branch_first, branch_second, branch_first_new, branch_second_new),
        (gate_first, gate_second, gate_first_new, gate_second_new),
    )
    for p, (first, second, first_new, second_new) in enumerate(both):
        moved, spread = moved_and_spread(projected[p], first[...], second[...])
        first_new[...] = moved
        second_new[...] = spread
    rows = (
        (branch_factor, branch_weight, branch_step, branch_new),
        (gate_factor, gate_weight, gate_step, gate_new),
    )
    for p, (factor, weight, step_out, new_out) in enumerate(rows):
        step = minus_scale * times_parts(factor[...], parts[p])
        step_out[...] = step
        new_out[...] = weight[...] + step


def outgoing_kernel(pieces, branch_weight, gate_weight, blocks):
    height = pieces.shape[1]
    block = branch_weight.shape[0]
    piece = jnp.sum(pieces[...], axis=0)
    for peer in range(blocks.shape[0]):
        blocks[peer, :height] = piece
        blocks[peer, height : height + block] = branch_weight[...]
        blocks[peer, height + block :] = gate_weight[...]


def total_kernel(mine, other, blocks):
    total = mine[...] + other[...]
    for peer in range(blocks.shape[0]):
        blocks[peer] = total


def totals(mine, other, peers):
    return pl.pallas_call(
        total_kernel,
        out_shape=jax.ShapeDtypeStruct((peers, *mine.shape), mine.dtype),
        in_specs=[whole()] * 2,
        out_specs=whole(),
        compiler_params=grant(2),
        name="totals",
    )(mine, other)


def factors_kernel(mine, other, factors):
    near_z, near_x, far, block, _ = mine.shape
    core = lax.axis_index("c")
    for f in range(far):
        for z in range(near_z):
            for x in range(near_x):
                row = ((f * near_z + z) * near_x + x) * 2 * block
                for source, place in ((mine, core), (other, 1 - core)):
                    rows = pl.ds(pl.multiple_of(row + place * block, block), block)
                    factors[rows, :] = source[z, x, f]


def placed(blocks, place, copies, done):
    near_z, near_x = blocks.shape[:2]
    width = copies[0].shape[-1]
    started = []
    for p, copy in enumerate(copies):
        for z in range(near_z):
            for x in range(near_x):
                started.append(
                    pltpu.make_async_copy(
                        blocks.at[z, x, :, :, pl.ds(p * width, width)],
                        copy.at[:, z, x, place],
                        done.at[len(started)],
                    )
                )
    for one in started:
        one.start()
    for one in started:
        one.wait()


def mine_kernel(mine, branch_copy, gate_copy, done):
    placed(mine, lax.axis_index("c"), (branch_copy, gate_copy), done)


def other_kernel(other, branch_in, gate_in, branch_copy, gate_copy, done):
    del branch_in, gate_in
    placed(other, 1 - lax.axis_index("c"), (branch_copy, gate_copy), done)


def whole():
    return pl.BlockSpec(memory_space=pltpu.VMEM)


def anywhere():
    return pl.BlockSpec(memory_space=pl.ANY)


def grant(mib):
    return pltpu.CompilerParams(vmem_limit_bytes=mib << 20)


def outgoing(pieces, branch_weight, gate_weight, peers):
    height = pieces.shape[1] + 2 * branch_weight.shape[0]
    return pl.pallas_call(
        outgoing_kernel,
        out_shape=jax.ShapeDtypeStruct((peers, height, pieces.shape[2]), jnp.float32),
        in_specs=[whole()] * 3,
        out_specs=whole(),
        compiler_params=grant(4),
        name="outgoing",
    )(pieces, branch_weight, gate_weight)


def whole_factors(mine, other):
    near_z, near_x, far, block, columns = mine.shape
    return pl.pallas_call(
        factors_kernel,
        out_shape=jax.ShapeDtypeStruct((2 * near_z * near_x * far * block, columns), mine.dtype),
        in_specs=[whole()] * 2,
        out_specs=whole(),
        compiler_params=grant(4),
        name="whole_factors",
    )(mine, other)


def copies_of(mine):
    near_z, near_x, far, block, columns = mine.shape
    copy = jax.ShapeDtypeStruct((far, near_z, near_x, 2, block, columns // 2), mine.dtype)
    return [copy, copy], [pltpu.SemaphoreType.DMA((2 * near_z * near_x,))]


def place_mine(mine):
    shapes, scratch = copies_of(mine)
    return pl.pallas_call(
        mine_kernel,
        out_shape=shapes,
        in_specs=[whole()],
        out_specs=[anywhere()] * 2,
        scratch_shapes=scratch,
        compiler_params=grant(4),
        cost_estimate=pl.CostEstimate(flops=1 << 20, bytes_accessed=1 << 21, transcendentals=0),
        name="place_mine",
    )(mine)


def place_other(other, branch_copy, gate_copy):
    shapes, scratch = copies_of(other)
    return pl.pallas_call(
        other_kernel,
        out_shape=shapes,
        in_specs=[whole(), anywhere(), anywhere()],
        out_specs=[anywhere()] * 2,
        scratch_shapes=scratch,
        input_output_aliases={1: 0, 2: 1},
        compiler_params=grant(4),
        name="place_other",
    )(other, branch_copy, gate_copy)


def directions(projected, branch_first, gate_first, branch_second, gate_second):
    rank, width = branch_first.shape
    return pl.pallas_call(
        direction_kernel,
        out_shape=[
            jax.ShapeDtypeStruct((2, rank, 3 * width), jnp.bfloat16),
            jax.ShapeDtypeStruct((8, 128), jnp.float32),
        ],
        in_specs=[whole()] * 5,
        out_specs=[whole()] * 2,
        compiler_params=grant(6),
        name="directions",
    )(projected, branch_first, gate_first, branch_second, gate_second)


def new_rows(entries, squares, parts, factors, mine, other, peers):
    far, block, _ = factors.shape
    return pl.pallas_call(
        functools.partial(rows_kernel, entries),
        out_shape=jax.ShapeDtypeStruct((peers, far, block, 2 * mine.shape[2]), jnp.bfloat16),
        in_specs=[whole()] * 5,
        out_specs=whole(),
        compiler_params=grant(6),
        name="new_rows",
    )(squares, parts, factors, mine, other)


def results(entries, projected, moments, squares, parts, factors, weights):
    rank, width = moments[0].shape
    block = weights[0].shape[0]
    row = jax.ShapeDtypeStruct((block, width), jnp.float32)
    moment = jax.ShapeDtypeStruct((rank, width), jnp.float32)
    return pl.pallas_call(
        functools.partial(results_kernel, entries),
        out_shape=[row] * 4 + [moment] * 4,
        in_specs=[whole()] * 11,
        out_specs=[whole()] * 8,
        compiler_params=grant(6),
        cost_estimate=pl.CostEstimate(flops=1 << 22, bytes_accessed=1 << 21, transcendentals=0),
        name="results",
    )(projected, *moments, squares, parts, *factors, *weights)


def body(
    layer_input,
    branch_cotangent,
    gate_cotangent,
    branch_factor,
    gate_factor,
    branch_weight,
    gate_weight,
    branch_first,
    gate_first,
    branch_second,
    gate_second,
):
    rank, width = branch_first.shape
    near = (lax.axis_size("zl"), lax.axis_size("x"))

    far_factors = from_everyone(jnp.concatenate([branch_factor, gate_factor], axis=1), FAR)
    near_factors = from_everyone(far_factors, NEAR).reshape(*near, *far_factors.shape)
    factors = whole_factors(near_factors, swapped(near_factors))

    rows = jnp.dot(layer_input, factors, preferred_element_type=jnp.float32)
    both = jnp.stack(
        [
            projected_locally(rows[:, :rank], branch_cotangent),
            projected_locally(rows[:, rank:], gate_cotangent),
        ]
    )
    pieces = both.reshape(size_of(NEAR_CORES), -1, width)
    height = pieces.shape[1]
    blocks = outgoing(
        exchanged(pieces, NEAR_CORES), branch_weight, gate_weight, lax.axis_size("zh")
    )
    arrived = exchanged(blocks, ("zh",))
    partial = arrived[:, :height].sum(axis=0)
    weights = arrived[:, height:]
    other_partial = swapped(partial, "zm")
    other_weights = swapped(weights, "zm")
    sums = totals(partial, other_partial, size_of(NEAR_CORES))
    projected = exchanged(sums, NEAR_CORES).reshape(both.shape)

    entries = 2 * rank * width * lax.axis_size("tp")
    moments = (branch_first, gate_first, branch_second, gate_second)
    parts, squares = directions(projected, *moments)
    squares = from_everyone(squares, ("tp",))
    rows_new = new_rows(
        entries, squares, parts, far_factors, weights, other_weights, size_of(NEAR)
    )

    mine = exchanged(rows_new, NEAR).reshape(*near, *rows_new.shape[1:])
    other = swapped(mine)
    copies = place_mine(mine)
    (
        branch_step,
        gate_step,
        branch_new,
        gate_new,
        branch_first_new,
        gate_first_new,
        branch_second_new,
        gate_second_new,
    ) = results(
        entries,
        projected,
        moments,
        squares,
        parts,
        (branch_factor, gate_factor),
        (branch_weight, gate_weight),
    )
    branch_copy, gate_copy = [c.reshape(-1, width) for c in place_other(other, *copies)]
    return (
        branch_step,
        gate_step,
        branch_new,
        gate_new,
        branch_copy,
        gate_copy,
        branch_first_new,
        gate_first_new,
        branch_second_new,
        gate_second_new,
    )


def solution(mesh):
    finer = Mesh(
        mesh.devices.reshape(4, 2, 2, 4, 2, mesh.shape["tp"]),
        ("zh", "zm", "zl", "x", "c", "tp"),
    )
    sharded = P(FS, None)
    split = P(FS, "tp")
    kept = P(None, "tp")
    in_specs = (sharded, split, split, sharded, sharded, split, split, kept, kept, kept, kept)
    out_specs = (split, split, split, split, kept, kept, kept, kept, kept, kept)
    return jax.shard_map(body, mesh=finer, in_specs=in_specs, out_specs=out_specs, check_vma=False)
```
